256 devices in a mesh: grp: 2 (over y), fs: 16 (over z), tp: 8 (over x, core).
Axes of the slice: x: 4, y: 2, z: 16, core: 2. Of those that a mesh axis runs over, the one named last changes fastest.
The devices are a block of a 4x16x16 slice.
Arguments:
- tokens: bfloat16 [24576, 2048], P(('grp', 'fs'), 'tp'), parts along dimension 0, may hold values from -6 to 6
- mix_gain: float32 [2048], replicated, may hold values from 0.1 to 1.9
- w_u: float32 [2048, 1024], P('fs', 'tp'), may hold values from -0.125 to 0.125
- w_v: float32 [2048, 1024], P('fs', 'tp'), may hold values from -0.125 to 0.125
- u_scale: float32 [1024], P('tp'), may hold values from 0.5 to 2
- v_scale: float32 [1024], P('tp'), may hold values from 0.5 to 2
- spatial: bfloat16 [8, 128, 128], P('tp'), may hold values from -0.5 to 0.5
- spatial_bias: float32 [8, 128], P('tp'), may hold values from 0.1 to 1.9
- w_mix: float32 [1024, 2048], P('tp', 'fs'), may hold values from -0.1875 to 0.1875
- mix_scale: float32 [1, 2048], P(None, 'fs'), may hold values from 0.5 to 2
- ffn_gain: float32 [2048], replicated, may hold values from 0.1 to 1.9
- w_gate: float32 [2048, 5632], P('fs', 'tp'), may hold values from -0.125 to 0.125
- w_up: float32 [2048, 5632], P('fs', 'tp'), may hold values from -0.125 to 0.125
- gate_scale: float32 [5632], P('tp'), may hold values from 0.5 to 2
- up_scale: float32 [5632], P('tp'), may hold values from 0.5 to 2
- w_down: float32 [5632, 2048], P('tp', 'fs'), may hold values from -0.078125 to 0.078125
- down_scale: float32 [1, 2048], P(None, 'fs'), may hold values from 0.5 to 2
Outputs:
- layer_out: bfloat16 [24576, 2048], P(('grp', 'fs'), 'tp'), parts along dimension 0
The draws below stay inside these ranges and needn't reach their ends.
There are 2 independent parts, one for each index of `grp`. The reference program is written for one: setup_inputs(seed, part) draws one part's arguments, and reference() takes and returns one part's arrays. A program takes and returns all parts, laid end to end along the dimension named above; an argument that names none is the same for every part. Nothing has to cross between parts.
All inputs are finite; a program needn't handle non-finite values.
Results may differ from the reference program's by a relative error of at most 0.024.
Values may be sent and summed in bfloat16 or wider, within the bound.
No kernel may reach another device: no remote copies, remote signals or barrier semaphores. Data moves between devices by JAX's collectives and lax.ppermute only.
A program may use at most 128 MiB of HBM per device.

```python
import math
import jax
import jax.numpy as jnp
from jax import lax

D = 2048
SGD = 128
SG = 8
SW = 1024
FF = 5632
BLK = 128
TOKENS = 12288
N_TP = 8


def shard_levels(key, dims, shards, least, high):
    loudness = 1.0
    for position, shards_of in shards:
        steps = jax.random.uniform(jax.random.fold_in(jax.random.fold_in(key, 6), position), (shards_of,), jnp.float32, least / len(shards), high / len(shards))
        loudness = loudness * jnp.repeat(jnp.exp(steps), dims[position] // shards_of).reshape((-1,) + (1,) * (len(dims) - 1 - position))
    return loudness


def centred(rng, shape, scale, limit, cuts=(), dtype=jnp.bfloat16):
    drawn = scale * jax.random.normal(rng, shape, jnp.float32)
    if cuts:
        drawn = drawn * shard_levels(rng, shape, cuts, -0.22, 0.18)
    return jnp.clip(drawn, -limit, limit).astype(dtype)


def setup_inputs(seed: int = 0, part: int = 0) -> dict:
    splits = jax.random.split(jax.random.key(seed), 18)
    part_keys = jax.random.split(jax.random.fold_in(splits[17], part), 18)
    return {
        "tokens": centred(part_keys[0], (TOKENS, D), 1.0, 6.0, ((0, 16), (1, 8))),
        "mix_gain": jnp.clip(1.0 + 0.18 * jax.random.normal(splits[1], (D,), jnp.float32), 0.1, 1.9),
        "w_u": centred(splits[2], (D, SW), D ** -0.5, 0.125, ((0, 16), (1, 8)), jnp.float32),
        "w_v": centred(splits[3], (D, SW), D ** -0.5, 0.125, ((0, 16), (1, 8)), jnp.float32),
        "u_scale": jnp.clip(jnp.exp(math.log(2.0) - 1.3862944 * jax.random.uniform(splits[4], (SW,), jnp.float32) ** shard_levels(splits[4], (SW,), ((0, 8),), -0.2, 0.2)), 0.5, 2.0),
        "v_scale": jnp.clip(jnp.exp(math.log(2.0) - 1.3862944 * jax.random.uniform(splits[5], (SW,), jnp.float32) ** shard_levels(splits[5], (SW,), ((0, 8),), -0.2, 0.2)), 0.5, 2.0),
        "spatial": centred(splits[6], (SG, BLK, BLK), BLK ** -0.5, 0.5, ((0, 8),)),
        "spatial_bias": jnp.clip(1.0 + 0.18 * jax.random.normal(splits[7], (SG, BLK), jnp.float32), 0.1, 1.9),
        "w_mix": centred(splits[8], (SW, D), SW ** -0.5, 0.1875, ((0, 8), (1, 16)), jnp.float32),
        "mix_scale": jnp.clip(jnp.exp(math.log(2.0) - 1.3862944 * jax.random.uniform(splits[9], (1, D), jnp.float32) ** shard_levels(splits[9], (1, D), ((1, 16),), -0.2, 0.2)), 0.5, 2.0),
        "ffn_gain": jnp.clip(1.0 + 0.18 * jax.random.normal(splits[10], (D,), jnp.float32), 0.1, 1.9),
        "w_gate": centred(splits[11], (D, FF), D ** -0.5, 0.125, ((0, 16), (1, 8)), jnp.float32),
        "w_up": centred(splits[12], (D, FF), D ** -0.5, 0.125, ((0, 16), (1, 8)), jnp.float32),
        "gate_scale": jnp.clip(jnp.exp(math.log(2.0) - 1.3862944 * jax.random.uniform(splits[13], (FF,), jnp.float32) ** shard_levels(splits[13], (FF,), ((0, 8),), -0.2, 0.2)), 0.5, 2.0),
        "up_scale": jnp.clip(jnp.exp(math.log(2.0) - 1.3862944 * jax.random.uniform(splits[14], (FF,), jnp.float32) ** shard_levels(splits[14], (FF,), ((0, 8),), -0.2, 0.2)), 0.5, 2.0),
        "w_down": centred(splits[15], (FF, D), FF ** -0.5, 0.078125, ((0, 8), (1, 16)), jnp.float32),
        "down_scale": jnp.clip(jnp.exp(math.log(2.0) - 1.3862944 * jax.random.uniform(splits[16], (1, D), jnp.float32) ** shard_levels(splits[16], (1, D), ((1, 16),), -0.2, 0.2)), 0.5, 2.0),
    }


eps = 1e-06

def norm_rows(rows, gain):
    wide = rows.astype(jnp.float32)
    factor = lax.rsqrt(lax.optimization_barrier(jnp.mean(wide * wide, axis=1, keepdims=True)) + eps)
    return (wide * factor * gain).astype(jnp.bfloat16)

def sliced_sum(hidden, weight, scale):
    width = hidden.shape[1] // N_TP
    total = jnp.zeros((hidden.shape[0], weight.shape[1]), jnp.float32)
    weight_half = weight.astype(jnp.bfloat16)
    for index in range(N_TP):
        left = hidden[:, index * width:(index + 1) * width]
        right = weight_half[index * width:(index + 1) * width]
        term = jnp.dot(left, right, preferred_element_type=jnp.float32) * scale
        rounded = lax.optimization_barrier(term.astype(jnp.bfloat16))
        total = total + rounded.astype(jnp.float32)
    return total

def reference(tokens, mix_gain, w_u, w_v, u_scale, v_scale, spatial, spatial_bias, w_mix, mix_scale, ffn_gain, w_gate, w_up, gate_scale, up_scale, w_down, down_scale):
    normed_in = norm_rows(tokens, mix_gain)
    u_act = jax.nn.gelu(jnp.dot(normed_in, w_u.astype(jnp.bfloat16), preferred_element_type=jnp.float32) * u_scale, approximate=False)
    v_act = jax.nn.gelu(jnp.dot(normed_in, w_v.astype(jnp.bfloat16), preferred_element_type=jnp.float32) * v_scale, approximate=False).astype(jnp.bfloat16)
    count = tokens.shape[0]
    blocks = v_act.reshape(count // BLK, BLK, SG, SGD).astype(jnp.float32)
    causal = jnp.arange(BLK)[:, None] >= jnp.arange(BLK)[None, :]
    masked = jnp.where(causal[None], spatial.astype(jnp.float32), jnp.float32(0.0))
    spatial_out = jnp.einsum('gts,nsgc->ntgc', masked, blocks) + spatial_bias.T[None, :, :, None]
    gated = (u_act * spatial_out.reshape(count, SW)).astype(jnp.bfloat16)
    mixed = sliced_sum(gated, w_mix, mix_scale)
    resid = (tokens.astype(jnp.float32) + mixed).astype(jnp.bfloat16)
    normed_ffn = norm_rows(resid, ffn_gain)
    gate_val = jnp.dot(normed_ffn, w_gate.astype(jnp.bfloat16), preferred_element_type=jnp.float32) * gate_scale
    up_val = jnp.dot(normed_ffn, w_up.astype(jnp.bfloat16), preferred_element_type=jnp.float32) * up_scale
    act = (jax.nn.silu(gate_val) * up_val).astype(jnp.bfloat16)
    down_sum = sliced_sum(act, w_down, down_scale)
    return (resid.astype(jnp.float32) + down_sum).astype(jnp.bfloat16)
```

```python
import functools

import jax
import jax.numpy as jnp
from jax import lax
from jax.experimental import pallas as pl
from jax.experimental.pallas import tpu as pltpu
from jax.sharding import PartitionSpec as P

eps = 1e-06
CORES = 2


def swap_cores(x):
    count = lax.axis_size("tp")
    return lax.ppermute(x, "tp", [(i, i ^ 1) for i in range(count)])


def to_chip(x, step):
    count = lax.axis_size("tp")
    return lax.ppermute(x, "tp", [(i, (i + CORES * step) % count) for i in range(count)])


def gather_features(shard):
    chips = lax.axis_size("tp") // CORES
    got = [shard]
    got += [to_chip(shard, step) for step in range(1, chips)]
    return [piece for g in got for piece in (g, swap_cores(g))]


def chunk_order(me, count):
    chips = count // CORES
    chip, core = lax.div(me, CORES), lax.rem(me, CORES)
    order = []
    for step in range(chips):
        source = CORES * lax.rem(chip + chips - step, chips)
        order += [source + core, source + 1 - core]
    return order


def target_order(me, count):
    chips = count // CORES
    chip, core = lax.div(me, CORES), lax.rem(me, CORES)
    chip_of = [CORES * lax.rem(chip + step, chips) for step in range(chips)]
    return [c + core for c in chip_of] + [c + 1 - core for c in chip_of]


def sum_shares(mine, theirs):
    other = swap_cores(theirs)
    chips = lax.axis_size("tp") // CORES
    pair = [mine[s].astype(jnp.float32) + other[s].astype(jnp.float32) for s in range(chips)]
    total = pair[0]
    for step in range(1, chips):
        total = total + to_chip(pair[step].astype(jnp.bfloat16), step).astype(jnp.float32)
    return total


def dot_f32(a, b, dims=(((1,), (0,)), ((), ()))):
    return lax.dot_general(a, b, dims, preferred_element_type=jnp.float32)


def pass_on(x, step):
    count = lax.axis_size("fs")
    return lax.ppermute(x, "fs", [(i, (i + step) % count) for i in range(count)])


class Ring:
    def __init__(self, shard):
        self.count = lax.axis_size("fs")
        self.ahead = self.behind = shard
        self.held = [shard]
        self.step = 0

    def advance(self):
        self.step += 1
        self.ahead = pass_on(self.ahead, 1)
        new = [self.ahead]
        if 2 * self.step < self.count:
            self.behind = pass_on(self.behind, -1)
            new.append(self.behind)
        self.held += new
        return new


def ring_order(me, count):
    order = [me]
    for step in range(1, count // 2 + 1):
        order.append(lax.rem(me + count - step, count))
        if 2 * step < count:
            order.append(lax.rem(me + step, count))
    return order


def lane_block(index, width):
    return pl.ds(pl.multiple_of(index * width, width), width)


def lay_out(pieces, places, buf):
    width = pieces[0].shape[1]
    for place, piece in zip(places, pieces):
        buf[:, lane_block(place, width)] = piece[...]


def take_rows(xs, places, rows, buf):
    width = xs[0].shape[1]
    squares = None
    for place, x_ref in zip(places, xs):
        x = x_ref[rows, :]
        buf[:, lane_block(place, width)] = x
        wide = x.astype(jnp.float32)
        sq = jnp.sum(wide * wide, axis=1, keepdims=True)
        squares = sq if squares is None else squares + sq
    return lax.rsqrt(squares * (1.0 / (len(xs) * width)) + eps)


def store_shares(value, weights, targets, rows, mine_ref, theirs_ref):
    half, _, width = mine_ref.shape
    for s, target in enumerate(targets):
        w = weights(lane_block(target, width))
        out = mine_ref if s < half else theirs_ref
        out[s % half, rows, :] = dot_f32(value, w).astype(jnp.bfloat16)


def gating_kernel(*refs, chunks, shards, tall):
    xs, ws = refs[:chunks], refs[chunks : chunks + shards]
    spatial_ref, bias_ref, mine_ref, theirs_ref, x_buf, in_buf, out_buf = refs[chunks + shards :]
    span = spatial_ref.shape[0]
    depth = ws[0].shape[0]
    sources, targets = chunk_order(lax.axis_index("tp"), chunks), target_order(lax.axis_index("tp"), chunks)
    for z, w in zip(ring_order(lax.axis_index("fs"), shards), ws):
        in_buf[lane_block(z, depth), :] = w[:, : 2 * span]
        out_buf[:, lane_block(z, w.shape[1] - 2 * span)] = w[:, 2 * span :]
    later = lax.broadcasted_iota(jnp.int32, (span, span), 0)
    earlier = lax.broadcasted_iota(jnp.int32, (span, span), 1)
    mixing = spatial_ref[...]
    mixing = jnp.where(later >= earlier, mixing, jnp.zeros_like(mixing))

    def block(i, carry):
        rows = pl.ds(pl.multiple_of(i * tall, tall), tall)
        factor = take_rows(xs, sources, rows, x_buf)
        pre = dot_f32(x_buf[...], in_buf[...]) * factor
        act = 0.5 * pre * (1.0 + lax.erf(pre * (0.5**0.5)))
        u = act[:, :span]
        v = act[:, span:].astype(jnp.bfloat16)
        gated = []
        for b in range(tall // span):
            at = slice(b * span, (b + 1) * span)
            placed = dot_f32(mixing, v[at]) + bias_ref[...]
            gated.append((u[at] * placed).astype(jnp.bfloat16))
        gated = jnp.concatenate(gated, axis=0)
        store_shares(gated, lambda at: out_buf[:, at], targets, rows, mine_ref, theirs_ref)
        return carry

    lax.fori_loop(0, xs[0].shape[0] // tall, block, 0)


def channel_kernel(*refs, chunks, shards, tall):
    xs, refs = refs[:chunks], refs[chunks:]
    first_ref, gate_scale_ref, up_scale_ref, refs = *refs[:3], refs[3:]
    down, refs = refs[:shards], refs[shards:]
    mine_ref, theirs_ref, x_buf, first_buf, down_buf, sems = refs
    lanes = first_ref.shape[2]
    hidden = down_buf.shape[0]
    copies = [
        pltpu.make_async_copy(
            first_ref.at[z], first_buf.at[:, z * lanes : (z + 1) * lanes], sems.at[z]
        )
        for z in range(shards)
    ]
    for copy in copies:
        copy.start()
    sources = chunk_order(lax.axis_index("tp"), chunks)
    targets = target_order(lax.axis_index("tp"), chunks)
    lay_out(down, ring_order(lax.axis_index("fs"), shards), down_buf)
    for copy in copies:
        copy.wait()
    across = (((1,), (1,)), ((), ()))

    def block(i, carry):
        rows = pl.ds(pl.multiple_of(i * tall, tall), tall)
        factor = take_rows(xs, sources, rows, x_buf)
        gate = dot_f32(x_buf[...], first_buf[:hidden, :], across) * factor * gate_scale_ref[...]
        up = dot_f32(x_buf[...], first_buf[hidden:, :], across) * factor * up_scale_ref[...]
        act = (gate / (1.0 + jnp.exp(-gate)) * up).astype(jnp.bfloat16)
        store_shares(act, lambda at: down_buf[:, at], targets, rows, mine_ref, theirs_ref)
        return carry

    lax.fori_loop(0, xs[0].shape[0] // tall, block, 0)


def gain_rows(gain_ref):
    row = gain_ref[pl.ds(lax.axis_index("fs"), 1), :]
    return jnp.broadcast_to(row, (row.shape[1], row.shape[1]))


def near_kernel(gain_ref, u_ref, v_ref, mix_ref, u_scale_ref, v_scale_ref, mix_scale_ref, out_ref):
    gain = gain_rows(gain_ref).T
    parts = [
        u_ref[...] * gain * u_scale_ref[...],
        v_ref[...] * gain * v_scale_ref[...],
        mix_ref[...] * mix_scale_ref[...],
    ]
    at = 0
    for part in parts:
        out_ref[:, at : at + part.shape[1]] = part.astype(jnp.bfloat16)
        at += part.shape[1]


def first_kernel(gain_ref, gate_ref, up_ref, out_ref):
    gain = gain_rows(gain_ref)[:1, :]
    hidden = gate_ref.shape[0]
    out_ref[:hidden, :] = (gate_ref[...] * gain).astype(jnp.bfloat16)
    out_ref[hidden:, :] = (up_ref[...] * gain).astype(jnp.bfloat16)


def fold(kernel, name, rows, columns, *operands):
    return pl.pallas_call(
        kernel,
        out_shape=jax.ShapeDtypeStruct((rows, columns), jnp.bfloat16),
        cost_estimate=pl.CostEstimate(
            flops=4 * rows * columns, bytes_accessed=2**20, transcendentals=0
        ),
        compiler_params=pltpu.CompilerParams(vmem_limit_bytes=4 * 2**20),
        name=name,
    )(*operands)


def call(kernel, name, operands, specs, chunks, shards, tall, scratch, flops, limit):
    rows, width = operands[0].shape
    half = chunks // CORES
    vmem = pl.BlockSpec(memory_space=pltpu.VMEM)
    return pl.pallas_call(
        functools.partial(kernel, chunks=chunks, shards=shards, tall=tall),
        in_specs=[vmem if spec is None else spec for spec in specs],
        out_specs=[vmem, vmem],
        out_shape=[jax.ShapeDtypeStruct((half, rows, width), jnp.bfloat16)] * 2,
        scratch_shapes=[
            pltpu.VMEM(shape, jnp.bfloat16) if isinstance(shape, tuple) else shape
            for shape in scratch
        ],
        compiler_params=pltpu.CompilerParams(vmem_limit_bytes=limit * 2**20),
        cost_estimate=pl.CostEstimate(flops=flops, bytes_accessed=2**20, transcendentals=0),
        name=name,
    )(*operands)


def gating(pieces, weights, spatial, bias):
    chunks, shards, tall = len(pieces), len(weights), 256
    rows, width = pieces[0].shape
    span = spatial.shape[0]
    model = chunks * width
    flops = 2 * rows * (model * 2 * span + span * span + span * model)
    scratch = [(tall, model), (model, 2 * span), (span, model)]
    operands = [*pieces, *weights, spatial, bias]
    specs = [None] * len(operands)
    return call(gating_kernel, "gating", operands, specs, chunks, shards, tall, scratch, flops, 16)


def channel(pieces, first, gate_scale, up_scale, down):
    chunks, shards, tall = len(pieces), len(down), 256
    rows, width = pieces[0].shape
    hidden = down[0].shape[0]
    model = chunks * width
    flops = 2 * rows * model * 3 * hidden
    scratch = [(tall, model), (2 * hidden, model), (hidden, model), pltpu.SemaphoreType.DMA((shards,))]
    operands = [*pieces, first, gate_scale, up_scale, *down]
    specs = [None] * len(operands)
    specs[chunks] = pl.BlockSpec(memory_space=pltpu.HBM)
    return call(channel_kernel, "channel", operands, specs, chunks, shards, tall, scratch, flops, 24)


def local(
    tokens,
    mix_gain,
    w_u,
    w_v,
    u_scale,
    v_scale,
    spatial,
    spatial_bias,
    w_mix,
    mix_scale,
    ffn_gain,
    w_gate,
    w_up,
    gate_scale,
    up_scale,
    w_down,
    down_scale,
):
    depth, span = w_u.shape
    bias = jnp.broadcast_to(spatial_bias[0][:, None], spatial.shape[1:])
    down = (w_down * down_scale).astype(jnp.bfloat16)
    gate_scale, up_scale, bias, down, w_u = lax.optimization_barrier(
        (gate_scale[None], up_scale[None], bias, down, w_u)
    )
    hidden, out = w_down.shape
    near = fold(
        near_kernel,
        "near",
        depth,
        2 * span + w_mix.shape[1],
        mix_gain.reshape(-1, depth),
        w_u,
        w_v,
        w_mix,
        u_scale[None],
        v_scale[None],
        mix_scale,
    )
    first = fold(
        first_kernel, "first", 2 * hidden, depth, ffn_gain.reshape(-1, depth), w_gate.T, w_up.T
    )
    first = lax.all_gather(first, "fs")

    near_ring = Ring(near)
    steps = near_ring.count // 2
    for _ in range(steps):
        near_ring.advance()
    down, _ = lax.optimization_barrier((down, near_ring.held[-1]))
    down_ring = Ring(down)
    for _ in range(steps):
        down_ring.advance()

    mine, theirs = gating(gather_features(tokens), near_ring.held, spatial[0], bias)
    resid = (tokens.astype(jnp.float32) + sum_shares(mine, theirs)).astype(jnp.bfloat16)
    mine, theirs = channel(
        gather_features(resid), first, gate_scale, up_scale, down_ring.held
    )
    return (resid.astype(jnp.float32) + sum_shares(mine, theirs)).astype(jnp.bfloat16)


def solution(mesh):
    placed = (
        P(("grp", "fs"), "tp"),
        P(),
        P("fs", "tp"),
        P("fs", "tp"),
        P("tp"),
        P("tp"),
        P("tp", None, None),
        P("tp", None),
        P("tp", "fs"),
        P(None, "fs"),
        P(),
        P("fs", "tp"),
        P("fs", "tp"),
        P("tp"),
        P("tp"),
        P("tp", "fs"),
        P(None, "fs"),
    )
    return jax.shard_map(
        local, mesh=mesh, in_specs=placed, out_specs=P(("grp", "fs"), "tp"), check_vma=False
    )
```

```python
import functools

import jax
import jax.numpy as jnp
from jax import lax
from jax.experimental import pallas as pl
from jax.experimental.pallas import tpu as pltpu
from jax.sharding import PartitionSpec as P

eps = 1e-06
CORES = 2


def swap_cores(x):
    count = lax.axis_size("tp")
    return lax.ppermute(x, "tp", [(i, i ^ 1) for i in range(count)])


def to_chip(x, step):
    count = lax.axis_size("tp")
    return lax.ppermute(x, "tp", [(i, (i + CORES * step) % count) for i in range(count)])


def gather_features(shard):
    chips = lax.axis_size("tp") // CORES
    got = [shard]
    got += [to_chip(shard, step) for step in range(1, chips)]
    return [piece for g in got for piece in (g, swap_cores(g))]


def chunk_order(me, count):
    chips = count // CORES
    chip, core = lax.div(me, CORES), lax.rem(me, CORES)
    order = []
    for step in range(chips):
        source = CORES * lax.rem(chip + chips - step, chips)
        order += [source + core, source + 1 - core]
    return order


def sum_shares(mine, theirs):
    other = swap_cores(theirs)
    chips = lax.axis_size("tp") // CORES
    pair = [mine[s].astype(jnp.float32) + other[s].astype(jnp.float32) for s in range(chips)]
    total = pair[0]
    for step in range(1, chips):
        total = total + to_chip(pair[step].astype(jnp.bfloat16), step).astype(jnp.float32)
    return total


def dot_f32(a, b, dims=(((1,), (0,)), ((), ()))):
    return lax.dot_general(a, b, dims, preferred_element_type=jnp.float32)


def pass_on(x, step):
    count = lax.axis_size("fs")
    return lax.ppermute(x, "fs", [(i, (i + step) % count) for i in range(count)])


class Ring:
    def __init__(self, shard):
        self.count = lax.axis_size("fs")
        self.ahead = self.behind = shard
        self.held = [shard]
        self.step = 0

    def advance(self):
        self.step += 1
        self.ahead = pass_on(self.ahead, 1)
        new = [self.ahead]
        if 2 * self.step < self.count:
            self.behind = pass_on(self.behind, -1)
            new.append(self.behind)
        self.held += new
        return new


def ring_order(me, count):
    order = [me]
    for step in range(1, count // 2 + 1):
        order.append(lax.rem(me + count - step, count))
        if 2 * step < count:
            order.append(lax.rem(me + step, count))
    return order


def swap_groups(x):
    count = lax.axis_size("grp")
    return lax.ppermute(x, "grp", [(i, i ^ 1) for i in range(count)])


def lane_block(index, width):
    return pl.ds(pl.multiple_of(index * width, width), width)


def lay_out(pieces, places, buf):
    width = pieces[0].shape[1]
    for place, piece in zip(places, pieces):
        buf[:, lane_block(place, width)] = piece[...]


def take_rows(xs, places, rows, buf):
    width = xs[0].shape[1]
    squares = None
    for place, x_ref in zip(places, xs):
        x = x_ref[rows, :]
        buf[:, lane_block(place, width)] = x
        wide = x.astype(jnp.float32)
        sq = jnp.sum(wide * wide, axis=1, keepdims=True)
        squares = sq if squares is None else squares + sq
    return lax.rsqrt(squares * (1.0 / (len(xs) * width)) + eps)


def store_shares(value, weights, chunks, rows, mine_ref, theirs_ref):
    width = mine_ref.shape[2]
    chips = chunks // CORES
    me = lax.axis_index("tp")
    chip, core = lax.div(me, CORES), lax.rem(me, CORES)

    def fill(ref, which):
        def share(step, carry):
            target = CORES * lax.rem(chip + step, chips) + which
            w = weights(lane_block(target, width))
            ref[step, rows, :] = dot_f32(value, w).astype(jnp.bfloat16)
            return carry

        lax.fori_loop(0, chips, share, 0)

    fill(mine_ref, core)
    fill(theirs_ref, 1 - core)


def gating_kernel(*refs, chunks, shards, tall):
    xs, ws = refs[:chunks], refs[chunks : chunks + shards]
    spatial_ref, bias_ref, mine_ref, theirs_ref, x_buf, in_buf, out_buf = refs[chunks + shards :]
    span = spatial_ref.shape[0]
    depth = ws[0].shape[0]
    sources = chunk_order(lax.axis_index("tp"), chunks)
    for z, w in zip(ring_order(lax.axis_index("fs"), shards), ws):
        in_buf[lane_block(z, depth), :] = w[:, : 2 * span]
        out_buf[:, lane_block(z, w.shape[1] - 2 * span)] = w[:, 2 * span :]
    later = lax.broadcasted_iota(jnp.int32, (span, span), 0)
    earlier = lax.broadcasted_iota(jnp.int32, (span, span), 1)
    mixing = spatial_ref[...]
    mixing = jnp.where(later >= earlier, mixing, jnp.zeros_like(mixing))

    def block(i, carry):
        rows = pl.ds(pl.multiple_of(i * tall, tall), tall)
        factor = take_rows(xs, sources, rows, x_buf)
        pre = dot_f32(x_buf[...], in_buf[...]) * factor
        act = 0.5 * pre * (1.0 + lax.erf(pre * (0.5**0.5)))
        u = act[:, :span]
        v = act[:, span:].astype(jnp.bfloat16)
        gated = []
        for b in range(tall // span):
            at = slice(b * span, (b + 1) * span)
            placed = dot_f32(mixing, v[at]) + bias_ref[...]
            gated.append((u[at] * placed).astype(jnp.bfloat16))
        gated = jnp.concatenate(gated, axis=0)
        store_shares(gated, lambda at: out_buf[:, at], chunks, rows, mine_ref, theirs_ref)
        return carry

    lax.fori_loop(0, xs[0].shape[0] // tall, block, 0)


def channel_kernel(*refs, chunks, shards, tall):
    xs, refs = refs[:chunks], refs[chunks:]
    gate_scale_ref, up_scale_ref, other_ref, refs = *refs[:3], refs[3:]
    ring, refs = refs[:shards], refs[shards:]
    others, refs = refs[:-6], refs[-6:]
    mine_ref, theirs_ref, x_buf, first_buf, down_buf, wide_buf = refs
    lanes = other_ref.shape[1]
    hidden = down_buf.shape[0]
    side = lax.rem(lax.axis_index("grp"), 2)
    sources = chunk_order(lax.axis_index("tp"), chunks)
    around = ring_order(lax.axis_index("fs"), shards)
    for z, piece in zip(around, ring):
        first_buf[side, :, lane_block(z, lanes)] = piece[:hidden, :]
        down_buf[:, lane_block(z, lanes)] = piece[hidden:, :]
    swapped = [(other_ref, 0)]
    for piece in others:
        swapped += [(piece, at) for at in range(0, piece.shape[0], hidden)]
    for z, (piece, at) in zip(around, swapped):
        first_buf[1 - side, :, lane_block(z, lanes)] = piece[at : at + hidden, :]
    across = (((1,), (1,)), ((), ()))

    def block(i, carry):
        rows = pl.ds(pl.multiple_of(i * tall, tall), tall)
        factor = take_rows(xs, sources, rows, x_buf)

        def project(which, carry):
            wide_buf[which] = dot_f32(x_buf[...], first_buf[which], across)
            return carry

        lax.fori_loop(0, 2, project, 0)
        gate = wide_buf[0] * factor * gate_scale_ref[...]
        up = wide_buf[1] * factor * up_scale_ref[...]
        act = (gate / (1.0 + jnp.exp(-gate)) * up).astype(jnp.bfloat16)
        store_shares(act, lambda at: down_buf[:, at], chunks, rows, mine_ref, theirs_ref)
        return carry

    lax.fori_loop(0, xs[0].shape[0] // tall, block, 0)


def gain_rows(gain_ref):
    row = gain_ref[pl.ds(lax.axis_index("fs"), 1), :]
    return jnp.broadcast_to(row, (row.shape[1], row.shape[1]))


def near_kernel(gain_ref, u_ref, v_ref, mix_ref, u_scale_ref, v_scale_ref, mix_scale_ref, out_ref):
    gain = gain_rows(gain_ref).T
    parts = [
        u_ref[...] * gain * u_scale_ref[...],
        v_ref[...] * gain * v_scale_ref[...],
        mix_ref[...] * mix_scale_ref[...],
    ]
    at = 0
    for part in parts:
        out_ref[:, at : at + part.shape[1]] = part.astype(jnp.bfloat16)
        at += part.shape[1]


def far_kernel(gain_ref, gate_ref, up_ref, down_ref, down_scale_ref, out_ref, other_ref):
    gain = gain_rows(gain_ref)[:1, :]
    hidden = gate_ref.shape[0]
    even = lax.rem(lax.axis_index("grp"), 2) == 0
    gate, up = gate_ref[...], up_ref[...]
    out_ref[:hidden, :] = (jnp.where(even, gate, up) * gain).astype(jnp.bfloat16)
    out_ref[hidden:, :] = (down_ref[...] * down_scale_ref[...]).astype(jnp.bfloat16)
    other_ref[...] = (jnp.where(even, up, gate) * gain).astype(jnp.bfloat16)


def fold(kernel, name, shapes, *operands):
    return pl.pallas_call(
        kernel,
        out_shape=[jax.ShapeDtypeStruct(shape, jnp.bfloat16) for shape in shapes],
        cost_estimate=pl.CostEstimate(flops=2**22, bytes_accessed=2**20, transcendentals=0),
        compiler_params=pltpu.CompilerParams(vmem_limit_bytes=4 * 2**20),
        name=name,
    )(*operands)


def call(kernel, name, operands, specs, chunks, shards, tall, scratch, flops, limit):
    rows, width = operands[0].shape
    half = chunks // CORES
    vmem = pl.BlockSpec(memory_space=pltpu.VMEM)
    return pl.pallas_call(
        functools.partial(kernel, chunks=chunks, shards=shards, tall=tall),
        in_specs=[vmem if spec is None else spec for spec in specs],
        out_specs=[vmem, vmem],
        out_shape=[jax.ShapeDtypeStruct((half, rows, width), jnp.bfloat16)] * 2,
        scratch_shapes=[
            pltpu.VMEM(shape, jnp.bfloat16) if isinstance(shape, tuple) else shape
            for shape in scratch
        ],
        compiler_params=pltpu.CompilerParams(vmem_limit_bytes=limit * 2**20),
        cost_estimate=pl.CostEstimate(flops=flops, bytes_accessed=2**20, transcendentals=0),
        name=name,
    )(*operands)


def gating(pieces, weights, spatial, bias):
    chunks, shards, tall = len(pieces), len(weights), 256
    rows, width = pieces[0].shape
    span = spatial.shape[0]
    model = chunks * width
    flops = 2 * rows * (model * 2 * span + span * span + span * model)
    scratch = [(tall, model), (model, 2 * span), (span, model)]
    operands = [*pieces, *weights, spatial, bias]
    specs = [None] * len(operands)
    return call(gating_kernel, "gating", operands, specs, chunks, shards, tall, scratch, flops, 16)


def channel(pieces, gate_scale, up_scale, other, ring, others):
    chunks, shards, tall = len(pieces), len(ring), 256
    rows, width = pieces[0].shape
    hidden = gate_scale.shape[1]
    model = chunks * width
    flops = 2 * rows * model * 3 * hidden
    scratch = [
        (tall, model),
        (2, hidden, model),
        (hidden, model),
        pltpu.VMEM((2, tall, hidden), jnp.float32),
    ]
    operands = [*pieces, gate_scale, up_scale, other, *ring, *others]
    specs = [None] * len(operands)
    return call(channel_kernel, "channel", operands, specs, chunks, shards, tall, scratch, flops, 24)


def local(
    tokens,
    mix_gain,
    w_u,
    w_v,
    u_scale,
    v_scale,
    spatial,
    spatial_bias,
    w_mix,
    mix_scale,
    ffn_gain,
    w_gate,
    w_up,
    gate_scale,
    up_scale,
    w_down,
    down_scale,
):
    depth, span = w_u.shape
    hidden, out = w_down.shape
    bias = jnp.broadcast_to(spatial_bias[0][:, None], spatial.shape[1:])
    gate_scale, up_scale, bias, w_u = lax.optimization_barrier(
        (gate_scale[None], up_scale[None], bias, w_u)
    )
    (near,) = fold(
        near_kernel,
        "near",
        [(depth, 2 * span + w_mix.shape[1])],
        mix_gain.reshape(-1, depth),
        w_u,
        w_v,
        w_mix,
        u_scale[None],
        v_scale[None],
        mix_scale,
    )
    far, other = fold(
        far_kernel,
        "far",
        [(2 * hidden, out), (hidden, depth)],
        ffn_gain.reshape(-1, depth),
        w_gate.T,
        w_up.T,
        w_down,
        down_scale,
    )

    near_ring = Ring(near)
    steps = near_ring.count // 2
    for _ in range(steps):
        near_ring.advance()
    far, _ = lax.optimization_barrier((far, near_ring.held[-1]))
    far_ring = Ring(far)
    others = []
    for _ in range(steps):
        new = [piece[:hidden] for piece in far_ring.advance()]
        others.append(swap_groups(jnp.concatenate(new, axis=0)))

    mine, theirs = gating(gather_features(tokens), near_ring.held, spatial[0], bias)
    resid = (tokens.astype(jnp.float32) + sum_shares(mine, theirs)).astype(jnp.bfloat16)
    mine, theirs = channel(
        gather_features(resid), gate_scale, up_scale, other, far_ring.held, others
    )
    return (resid.astype(jnp.float32) + sum_shares(mine, theirs)).astype(jnp.bfloat16)


def solution(mesh):
    placed = (
        P(("grp", "fs"), "tp"),
        P(),
        P("fs", "tp"),
        P("fs", "tp"),
        P("tp"),
        P("tp"),
        P("tp", None, None),
        P("tp", None),
        P("tp", "fs"),
        P(None, "fs"),
        P(),
        P("fs", "tp"),
        P("fs", "tp"),
        P("tp"),
        P("tp"),
        P("tp", "fs"),
        P(None, "fs"),
    )
    return jax.shard_map(
        local, mesh=mesh, in_specs=placed, out_specs=P(("grp", "fs"), "tp"), check_vma=False
    )
```

```python
import functools

import jax
import jax.numpy as jnp
from jax import lax
from jax.experimental import pallas as pl
from jax.experimental.pallas import tpu as pltpu
from jax.sharding import PartitionSpec as P

eps = 1e-06
CORES = 2


def swap_cores(x):
    count = lax.axis_size("tp")
    return lax.ppermute(x, "tp", [(i, i ^ 1) for i in range(count)])


def to_chip(x, step):
    count = lax.axis_size("tp")
    return lax.ppermute(x, "tp", [(i, (i + CORES * step) % count) for i in range(count)])


def gather_features(shard):
    chips = lax.axis_size("tp") // CORES
    got = [shard]
    got += [to_chip(shard, step) for step in range(1, chips)]
    return [piece for g in got for piece in (g, swap_cores(g))]


def chunk_order(me, count):
    chips = count // CORES
    chip, core = lax.div(me, CORES), lax.rem(me, CORES)
    order = []
    for step in range(chips):
        source = CORES * lax.rem(chip + chips - step, chips)
        order += [source + core, source + 1 - core]
    return order


def chip_sums(mine, theirs):
    other = swap_cores(theirs)
    chips = lax.axis_size("tp") // CORES
    pair = [mine[s].astype(jnp.float32) + other[s].astype(jnp.float32) for s in range(chips)]
    return [pair[0]] + [p.astype(jnp.bfloat16) for p in pair[1:]]


def sum_chips(pair):
    total = pair[0]
    for step, p in enumerate(pair[1:], 1):
        total = total + to_chip(p, step).astype(jnp.float32)
    return total


def dot_f32(a, b, dims=(((1,), (0,)), ((), ()))):
    return lax.dot_general(a, b, dims, preferred_element_type=jnp.float32)


def pass_on(x, step):
    count = lax.axis_size("fs")
    return lax.ppermute(x, "fs", [(i, (i + step) % count) for i in range(count)])


class Ring:
    def __init__(self, shard):
        self.count = lax.axis_size("fs")
        self.ahead = self.behind = shard
        self.held = [shard]
        self.step = 0

    def after(self, *others):
        self.ahead, self.behind, *_ = lax.optimization_barrier((self.ahead, self.behind, *others))

    def advance(self):
        self.step += 1
        self.ahead = pass_on(self.ahead, 1)
        new = [self.ahead]
        if 2 * self.step < self.count:
            self.behind = pass_on(self.behind, -1)
            new.append(self.behind)
        self.held += new
        return new


def ring_order(me, count):
    order = [me]
    for step in range(1, count // 2 + 1):
        order.append(lax.rem(me + count - step, count))
        if 2 * step < count:
            order.append(lax.rem(me + step, count))
    return order


def swap_groups(x):
    count = lax.axis_size("grp")
    return lax.ppermute(x, "grp", [(i, i ^ 1) for i in range(count)])


def lane_block(index, width):
    return pl.ds(pl.multiple_of(index * width, width), width)


def lay_out(pieces, places, buf):
    width = pieces[0].shape[1]
    for place, piece in zip(places, pieces):
        buf[:, lane_block(place, width)] = piece[...]


def take_rows(xs, places, rows, buf):
    width = xs[0].shape[1]
    squares = None
    for place, x_ref in zip(places, xs):
        x = x_ref[rows, :]
        buf[:, lane_block(place, width)] = x
        wide = x.astype(jnp.float32)
        sq = jnp.sum(wide * wide, axis=1, keepdims=True)
        squares = sq if squares is None else squares + sq
    return lax.rsqrt(squares * (1.0 / (len(xs) * width)) + eps)


def store_shares(value, weights, chunks, rows, mine_ref, theirs_ref):
    width = mine_ref.shape[2]
    chips = chunks // CORES
    me = lax.axis_index("tp")
    chip, core = lax.div(me, CORES), lax.rem(me, CORES)

    def fill(ref, which):
        def share(step, carry):
            target = CORES * lax.rem(chip + step, chips) + which
            w = weights(lane_block(target, width))
            ref[step, rows, :] = dot_f32(value, w).astype(jnp.bfloat16)
            return carry

        lax.fori_loop(0, chips, share, 0)

    fill(mine_ref, core)
    fill(theirs_ref, 1 - core)


def gating_kernel(*refs, chunks, shards, tall):
    xs, ws = refs[:chunks], refs[chunks : chunks + shards]
    spatial_ref, bias_ref, mine_ref, theirs_ref, x_buf, in_buf, out_buf = refs[chunks + shards :]
    span = spatial_ref.shape[0]
    depth = ws[0].shape[0]
    sources = chunk_order(lax.axis_index("tp"), chunks)
    for z, w in zip(ring_order(lax.axis_index("fs"), shards), ws):
        in_buf[lane_block(z, depth), :] = w[:, : 2 * span]
        out_buf[:, lane_block(z, w.shape[1] - 2 * span)] = w[:, 2 * span :]
    later = lax.broadcasted_iota(jnp.int32, (span, span), 0)
    earlier = lax.broadcasted_iota(jnp.int32, (span, span), 1)
    bias = jnp.broadcast_to(bias_ref[...], (span, span)).T
    mixing = spatial_ref[...]
    mixing = jnp.where(later >= earlier, mixing, jnp.zeros_like(mixing))

    def block(i, carry):
        rows = pl.ds(pl.multiple_of(i * tall, tall), tall)
        factor = take_rows(xs, sources, rows, x_buf)
        pre = dot_f32(x_buf[...], in_buf[...]) * factor
        act = 0.5 * pre * (1.0 + lax.erf(pre * (0.5**0.5)))
        u = act[:, :span]
        v = act[:, span:].astype(jnp.bfloat16)
        gated = []
        for b in range(tall // span):
            at = slice(b * span, (b + 1) * span)
            placed = dot_f32(mixing, v[at]) + bias
            gated.append((u[at] * placed).astype(jnp.bfloat16))
        gated = jnp.concatenate(gated, axis=0)
        store_shares(gated, lambda at: out_buf[:, at], chunks, rows, mine_ref, theirs_ref)
        return carry

    lax.fori_loop(0, xs[0].shape[0] // tall, block, 0)


def channel_kernel(*refs, chunks, shards, tall):
    xs, refs = refs[:chunks], refs[chunks:]
    gate_scale_ref, up_scale_ref, other_ref, refs = *refs[:3], refs[3:]
    ring, refs = refs[:shards], refs[shards:]
    others, refs = refs[:-6], refs[-6:]
    mine_ref, theirs_ref, x_buf, first_buf, down_buf, wide_buf = refs
    lanes = other_ref.shape[1]
    hidden = down_buf.shape[0]
    side = lax.rem(lax.axis_index("grp"), 2)
    sources = chunk_order(lax.axis_index("tp"), chunks)
    around = ring_order(lax.axis_index("fs"), shards)
    for z, piece in zip(around, ring):
        first_buf[side, :, lane_block(z, lanes)] = piece[:hidden, :]
        down_buf[:, lane_block(z, lanes)] = piece[hidden:, :]
    swapped = [(other_ref, 0)]
    for piece in others:
        swapped += [(piece, at) for at in range(0, piece.shape[0], hidden)]
    for z, (piece, at) in zip(around, swapped):
        first_buf[1 - side, :, lane_block(z, lanes)] = piece[at : at + hidden, :]
    across = (((1,), (1,)), ((), ()))

    def block(i, carry):
        rows = pl.ds(pl.multiple_of(i * tall, tall), tall)
        factor = take_rows(xs, sources, rows, x_buf)

        def project(which, carry):
            wide_buf[which] = dot_f32(x_buf[...], first_buf[which], across)
            return carry

        lax.fori_loop(0, 2, project, 0)
        gate = wide_buf[0] * factor * gate_scale_ref[...][None, :]
        up = wide_buf[1] * factor * up_scale_ref[...][None, :]
        act = (gate / (1.0 + jnp.exp(-gate)) * up).astype(jnp.bfloat16)
        store_shares(act, lambda at: down_buf[:, at], chunks, rows, mine_ref, theirs_ref)
        return carry

    lax.fori_loop(0, xs[0].shape[0] // tall, block, 0)


def gain_rows(gain_ref):
    row = gain_ref[pl.ds(lax.axis_index("fs"), 1), :]
    return jnp.broadcast_to(row, (row.shape[1], row.shape[1]))


def fold_kernel(
    in_gain_ref,
    u_ref,
    v_ref,
    mix_ref,
    u_scale_ref,
    v_scale_ref,
    mix_scale_ref,
    mid_gain_ref,
    gate_ref,
    up_ref,
    down_ref,
    down_scale_ref,
    near_ref,
    far_ref,
    other_ref,
):
    gain = gain_rows(in_gain_ref).T
    parts = [
        u_ref[...] * gain * u_scale_ref[...],
        v_ref[...] * gain * v_scale_ref[...],
        mix_ref[...] * mix_scale_ref[...],
    ]
    at = 0
    for part in parts:
        near_ref[:, at : at + part.shape[1]] = part.astype(jnp.bfloat16)
        at += part.shape[1]
    gain = gain_rows(mid_gain_ref)[:1, :]
    hidden = gate_ref.shape[0]
    even = lax.rem(lax.axis_index("grp"), 2) == 0
    gate, up = gate_ref[...], up_ref[...]
    far_ref[:hidden, :] = (jnp.where(even, gate, up) * gain).astype(jnp.bfloat16)
    far_ref[hidden:, :] = (down_ref[...] * down_scale_ref[...]).astype(jnp.bfloat16)
    other_ref[...] = (jnp.where(even, up, gate) * gain).astype(jnp.bfloat16)


def fold(shapes, *operands):
    return pl.pallas_call(
        fold_kernel,
        grid=(1,),
        in_specs=[pl.BlockSpec(a.shape, lambda i: (0, 0)) for a in operands],
        out_specs=[pl.BlockSpec(memory_space=pltpu.VMEM)] * len(shapes),
        out_shape=[jax.ShapeDtypeStruct(shape, jnp.bfloat16) for shape in shapes],
        cost_estimate=pl.CostEstimate(flops=2**22, bytes_accessed=2**20, transcendentals=0),
        compiler_params=pltpu.CompilerParams(vmem_limit_bytes=60 * 2**20),
        name="fold",
    )(*operands)


def call(kernel, name, operands, specs, chunks, shards, tall, scratch, flops, limit):
    rows, width = operands[0].shape
    half = chunks // CORES
    vmem = pl.BlockSpec(memory_space=pltpu.VMEM)
    return pl.pallas_call(
        functools.partial(kernel, chunks=chunks, shards=shards, tall=tall),
        in_specs=[vmem if spec is None else spec for spec in specs],
        out_specs=[vmem, vmem],
        out_shape=[jax.ShapeDtypeStruct((half, rows, width), jnp.bfloat16)] * 2,
        scratch_shapes=[
            pltpu.VMEM(shape, jnp.bfloat16) if isinstance(shape, tuple) else shape
            for shape in scratch
        ],
        compiler_params=pltpu.CompilerParams(vmem_limit_bytes=limit * 2**20),
        cost_estimate=pl.CostEstimate(flops=flops, bytes_accessed=2**20, transcendentals=0),
        name=name,
    )(*operands)


def gating(pieces, weights, spatial, bias):
    chunks, shards, tall = len(pieces), len(weights), 256
    rows, width = pieces[0].shape
    span = spatial.shape[0]
    model = chunks * width
    flops = 2 * rows * (model * 2 * span + span * span + span * model)
    scratch = [(tall, model), (model, 2 * span), (span, model)]
    operands = [*pieces, *weights, spatial, bias]
    specs = [None] * len(operands)
    return call(gating_kernel, "gating", operands, specs, chunks, shards, tall, scratch, flops, 16)


def channel(pieces, gate_scale, up_scale, other, ring, others):
    chunks, shards, tall = len(pieces), len(ring), 256
    rows, width = pieces[0].shape
    hidden = gate_scale.shape[0]
    model = chunks * width
    flops = 2 * rows * model * 3 * hidden
    scratch = [
        (tall, model),
        (2, hidden, model),
        (hidden, model),
        pltpu.VMEM((2, tall, hidden), jnp.float32),
    ]
    operands = [*pieces, gate_scale, up_scale, other, *ring, *others]
    specs = [None] * len(operands)
    return call(channel_kernel, "channel", operands, specs, chunks, shards, tall, scratch, flops, 24)


def local(
    tokens,
    mix_gain,
    w_u,
    w_v,
    u_scale,
    v_scale,
    spatial,
    spatial_bias,
    w_mix,
    mix_scale,
    ffn_gain,
    w_gate,
    w_up,
    gate_scale,
    up_scale,
    w_down,
    down_scale,
):
    depth, span = w_u.shape
    hidden, out = w_down.shape
    near, far, other = fold(
        [(depth, 2 * span + w_mix.shape[1]), (2 * hidden, out), (hidden, depth)],
        mix_gain.reshape(-1, depth),
        w_u,
        w_v,
        w_mix,
        u_scale[None],
        v_scale[None],
        mix_scale,
        ffn_gain.reshape(-1, depth),
        w_gate.T,
        w_up.T,
        w_down,
        down_scale,
    )

    near_ring = Ring(near)
    steps = near_ring.count // 2
    for _ in range(steps):
        near_ring.advance()
    far_ring = Ring(far)
    far_ring.after(near_ring.held[-1])
    others = []

    def go_round():
        if len(others) > 1:
            far_ring.after(others[-2])
        new = [piece[:hidden] for piece in far_ring.advance()]
        others.append(swap_groups(jnp.concatenate(new, axis=0)))

    mine, theirs = gating(gather_features(tokens), near_ring.held, spatial[0], spatial_bias)
    go_round()
    pair = chip_sums(mine, theirs)
    far_ring.after(*pair[1:])
    go_round()
    go_round()
    resid = (tokens.astype(jnp.float32) + sum_chips(pair)).astype(jnp.bfloat16)
    far_ring.after(resid)
    for _ in range(steps - 3):
        go_round()
    pieces = gather_features(resid)
    mine, theirs = channel(pieces, gate_scale, up_scale, other, far_ring.held, others)
    pair = chip_sums(mine, theirs)
    return (resid.astype(jnp.float32) + sum_chips(pair)).astype(jnp.bfloat16)


def solution(mesh):
    placed = (
        P(("grp", "fs"), "tp"),
        P(),
        P("fs", "tp"),
        P("fs", "tp"),
        P("tp"),
        P("tp"),
        P("tp", None, None),
        P("tp", None),
        P("tp", "fs"),
        P(None, "fs"),
        P(),
        P("fs", "tp"),
        P("fs", "tp"),
        P("tp"),
        P("tp"),
        P("tp", "fs"),
        P(None, "fs"),
    )
    return jax.shard_map(
        local, mesh=mesh, in_specs=placed, out_specs=P(("grp", "fs"), "tp"), check_vma=False
    )
```

```python
import functools

import jax
import jax.numpy as jnp
from jax import lax
from jax.experimental import pallas as pl
from jax.experimental.pallas import tpu as pltpu
from jax.sharding import PartitionSpec as P

eps = 1e-06
CORES = 2


def swap_cores(x):
    count = lax.axis_size("tp")
    return lax.ppermute(x, "tp", [(i, i ^ 1) for i in range(count)])


def to_chip(x, step):
    count = lax.axis_size("tp")
    return lax.ppermute(x, "tp", [(i, (i + CORES * step) % count) for i in range(count)])


def gather_features(shard):
    chips = lax.axis_size("tp") // CORES
    got = [to_chip(shard, step) for step in range(1, chips)]
    near = swap_cores(jnp.stack([got[0], got[-1]]))
    swapped = [near[0], *[swap_cores(g) for g in got[1:-1]], near[1]]
    return [shard, swap_cores(shard), *[p for pair in zip(got, swapped) for p in pair]]


def chunk_order(me, count):
    chips = count // CORES
    chip, core = lax.div(me, CORES), lax.rem(me, CORES)
    order = []
    for step in range(chips):
        source = CORES * lax.rem(chip + chips - step, chips)
        order += [source + core, source + 1 - core]
    return order


def chip_sums(mine, theirs):
    other = swap_cores(theirs)
    chips = lax.axis_size("tp") // CORES
    pair = [mine[s].astype(jnp.float32) + other[s].astype(jnp.float32) for s in range(chips)]
    return [pair[0]] + [p.astype(jnp.bfloat16) for p in pair[1:]]


def sum_chips(pair):
    total = pair[0]
    for step, p in enumerate(pair[1:], 1):
        total = total + to_chip(p, step).astype(jnp.float32)
    return total


def dot_f32(a, b, dims=(((1,), (0,)), ((), ()))):
    return lax.dot_general(a, b, dims, preferred_element_type=jnp.float32)


def pass_on(x, step):
    count = lax.axis_size("fs")
    return lax.ppermute(x, "fs", [(i, (i + step) % count) for i in range(count)])


class Ring:
    def __init__(self, shard):
        self.count = lax.axis_size("fs")
        self.ahead = self.behind = shard
        self.held = [shard]
        self.before = [shard, shard]
        self.step = 0

    def after(self, *others):
        self.ahead, *_ = lax.optimization_barrier((self.ahead, *others))

    def advance(self):
        self.step += 1
        before, self.before = self.before, [self.ahead, self.behind]
        self.ahead, _ = lax.optimization_barrier((self.ahead, before[1]))
        self.behind, _ = lax.optimization_barrier((self.behind, before[0]))
        self.ahead = pass_on(self.ahead, 1)
        new = [self.ahead]
        if 2 * self.step < self.count:
            self.behind = pass_on(self.behind, -1)
            new.append(self.behind)
        self.held += new
        return new


def ring_order(me, count):
    order = [me]
    for step in range(1, count // 2 + 1):
        order.append(lax.rem(me + count - step, count))
        if 2 * step < count:
            order.append(lax.rem(me + step, count))
    return order


def lane_block(index, width):
    return pl.ds(pl.multiple_of(index * width, width), width)


def copy_all(pairs, sems, base):
    copies = [
        pltpu.make_async_copy(source, target, sems.at[base + i])
        for i, (source, target) in enumerate(pairs)
    ]
    for copy in copies:
        copy.start()

    def wait():
        for copy in copies:
            copy.wait()

    return wait, base + len(copies)


def load_rows(xs, buf, sems, base):
    width = xs[0].shape[1]
    places = chunk_order(lax.axis_index("tp"), len(xs))
    return copy_all(
        [(x, buf.at[:, lane_block(place, width)]) for x, place in zip(xs, places)], sems, base
    )


def row_factor(x):
    wide = x.astype(jnp.float32)
    return lax.rsqrt(jnp.mean(wide * wide, axis=1, keepdims=True) + eps)


def store_shares(value, weights, chunks, rows, mine_ref, theirs_ref):
    width = mine_ref.shape[2]
    chips = chunks // CORES
    me = lax.axis_index("tp")
    chip, core = lax.div(me, CORES), lax.rem(me, CORES)

    def fill(ref, which):
        def share(step, carry):
            target = CORES * lax.rem(chip + step, chips) + which
            w = weights(lane_block(target, width))
            ref[step, rows, :] = dot_f32(value, w).astype(jnp.bfloat16)
            return carry

        lax.fori_loop(0, chips, share, 0)

    fill(mine_ref, core)
    fill(theirs_ref, 1 - core)


def gating_kernel(*refs, chunks, shards, tall):
    xs, refs = refs[:chunks], refs[chunks:]
    near_ref, spatial_ref, bias_ref, mine_ref, theirs_ref, x_buf, in_buf, out_buf, sems = refs
    span = spatial_ref.shape[0]
    lanes = near_ref.shape[2] - 2 * span
    x_here, at = load_rows(xs, x_buf, sems, 0)
    in_here, at = copy_all([(near_ref.at[:, :, : 2 * span], in_buf)], sems, at)
    out_here, at = copy_all(
        [
            (near_ref.at[z, :, 2 * span :], out_buf.at[:, z * lanes : (z + 1) * lanes])
            for z in range(shards)
        ],
        sems,
        at,
    )
    later = lax.broadcasted_iota(jnp.int32, (span, span), 0)
    earlier = lax.broadcasted_iota(jnp.int32, (span, span), 1)
    bias = jnp.broadcast_to(bias_ref[...], (span, span)).T
    mixing = spatial_ref[...]
    mixing = jnp.where(later >= earlier, mixing, jnp.zeros_like(mixing))
    x_here()
    in_here()
    out_here()

    def block(i, carry):
        rows = pl.ds(pl.multiple_of(i * tall, tall), tall)
        x = x_buf[rows, :]
        weights = in_buf[...].reshape(x.shape[1], 2 * span)
        pre = dot_f32(x, weights) * row_factor(x)
        act = 0.5 * pre * (1.0 + lax.erf(pre * (0.5**0.5)))
        u = act[:, :span]
        v = act[:, span:].astype(jnp.bfloat16)
        gated = []
        for b in range(tall // span):
            at = slice(b * span, (b + 1) * span)
            placed = dot_f32(mixing, v[at]) + bias
            gated.append((u[at] * placed).astype(jnp.bfloat16))
        gated = jnp.concatenate(gated, axis=0)
        store_shares(gated, lambda at: out_buf[:, at], chunks, rows, mine_ref, theirs_ref)
        return carry

    lax.fori_loop(0, xs[0].shape[0] // tall, block, 0)


def channel_kernel(*refs, chunks, shards, tall):
    xs, refs = refs[:chunks], refs[chunks:]
    gate_scale_ref, up_scale_ref, refs = *refs[:2], refs[2:]
    ring, refs = refs[:shards], refs[shards:]
    mine_ref, theirs_ref, x_buf, gate_buf, up_buf, down_buf, sems = refs
    lanes = ring[0].shape[1]
    hidden = down_buf.shape[0]
    around = ring_order(lax.axis_index("fs"), shards)

    def load(part, buf, base):
        rows = slice(part * hidden, (part + 1) * hidden)
        return copy_all(
            [(w.at[rows, :], buf.at[:, lane_block(z, lanes)]) for z, w in zip(around, ring)],
            sems,
            base,
        )

    x_here, at = load_rows(xs, x_buf, sems, 0)
    gate_here, at = load(0, gate_buf, at)
    up_here, at = load(1, up_buf, at)
    down_here, at = load(2, down_buf, at)
    across = (((1,), (1,)), ((), ()))
    x_here()
    gate_here()
    up_here()
    down_here()

    def block(i, carry):
        rows = pl.ds(pl.multiple_of(i * tall, tall), tall)
        x = x_buf[rows, :]
        factor = row_factor(x)
        gate = dot_f32(x, gate_buf[...], across) * factor * gate_scale_ref[...][None, :]
        up = dot_f32(x, up_buf[...], across) * factor * up_scale_ref[...][None, :]
        act = (gate / (1.0 + jnp.exp(-gate)) * up).astype(jnp.bfloat16)
        store_shares(act, lambda at: down_buf[:, at], chunks, rows, mine_ref, theirs_ref)
        return carry

    lax.fori_loop(0, xs[0].shape[0] // tall, block, 0)


def gain_rows(gain_ref):
    row = gain_ref[pl.ds(lax.axis_index("fs"), 1), :]
    return jnp.broadcast_to(row, (row.shape[1], row.shape[1]))


def fold_kernel(
    in_gain_ref,
    u_ref,
    v_ref,
    mix_ref,
    u_scale_ref,
    v_scale_ref,
    mix_scale_ref,
    mid_gain_ref,
    gate_ref,
    up_ref,
    down_ref,
    down_scale_ref,
    near_ref,
    far_ref,
):
    gain = gain_rows(in_gain_ref).T
    parts = [
        u_ref[...] * gain * u_scale_ref[...],
        v_ref[...] * gain * v_scale_ref[...],
        mix_ref[...] * mix_scale_ref[...],
    ]
    at = 0
    for part in parts:
        near_ref[:, at : at + part.shape[1]] = part.astype(jnp.bfloat16)
        at += part.shape[1]
    gain = gain_rows(mid_gain_ref)[:1, :]
    hidden = gate_ref.shape[0]
    far_ref[:hidden, :] = (gate_ref[...] * gain).astype(jnp.bfloat16)
    far_ref[hidden : 2 * hidden, :] = (up_ref[...] * gain).astype(jnp.bfloat16)
    far_ref[2 * hidden :, :] = (down_ref[...] * down_scale_ref[...]).astype(jnp.bfloat16)


def fold(shapes, *operands):
    return pl.pallas_call(
        fold_kernel,
        grid=(1,),
        in_specs=[pl.BlockSpec(a.shape, lambda i: (0, 0)) for a in operands],
        out_specs=[pl.BlockSpec(memory_space=pltpu.VMEM)] * len(shapes),
        out_shape=[jax.ShapeDtypeStruct(shape, jnp.bfloat16) for shape in shapes],
        cost_estimate=pl.CostEstimate(flops=2**22, bytes_accessed=2**20, transcendentals=0),
        compiler_params=pltpu.CompilerParams(vmem_limit_bytes=60 * 2**20),
        name="fold",
    )(*operands)


def call(kernel, name, operands, specs, chunks, shards, tall, scratch, flops, limit):
    rows, width = operands[0].shape
    half = chunks // CORES
    vmem = pl.BlockSpec(memory_space=pltpu.VMEM)
    return pl.pallas_call(
        functools.partial(kernel, chunks=chunks, shards=shards, tall=tall),
        in_specs=[vmem if spec is None else spec for spec in specs],
        out_specs=[vmem, vmem],
        out_shape=[jax.ShapeDtypeStruct((half, rows, width), jnp.bfloat16)] * 2,
        scratch_shapes=[
            pltpu.VMEM(shape, jnp.bfloat16) if isinstance(shape, tuple) else shape
            for shape in scratch
        ],
        compiler_params=pltpu.CompilerParams(vmem_limit_bytes=limit * 2**20),
        cost_estimate=pl.CostEstimate(flops=flops, bytes_accessed=2**20, transcendentals=0),
        name=name,
    )(*operands)


def gating(pieces, near, spatial, bias):
    chunks, shards, tall = len(pieces), near.shape[0], 256
    rows, width = pieces[0].shape
    span = spatial.shape[0]
    model = chunks * width
    flops = 2 * rows * (model * 2 * span + span * span + span * model)
    scratch = [
        (rows, model),
        (shards, model // shards, 2 * span),
        (span, model),
        pltpu.SemaphoreType.DMA((chunks + 1 + shards,)),
    ]
    operands = [*pieces, near, spatial, bias]
    specs = [pl.BlockSpec(memory_space=pl.ANY)] * (chunks + 1) + [None] * 2
    return call(gating_kernel, "gating", operands, specs, chunks, shards, tall, scratch, flops, 16)


def channel(pieces, gate_scale, up_scale, ring):
    chunks, shards, tall = len(pieces), len(ring), 256
    rows, width = pieces[0].shape
    hidden = gate_scale.shape[0]
    model = chunks * width
    flops = 2 * rows * model * 3 * hidden
    scratch = [(rows, model), *[(hidden, model)] * 3]
    scratch.append(pltpu.SemaphoreType.DMA((chunks + 3 * shards,)))
    operands = [*pieces, gate_scale, up_scale, *ring]
    specs = [pl.BlockSpec(memory_space=pl.ANY)] * len(operands)
    specs[chunks] = specs[chunks + 1] = None
    return call(channel_kernel, "channel", operands, specs, chunks, shards, tall, scratch, flops, 57)


def local(
    tokens,
    mix_gain,
    w_u,
    w_v,
    u_scale,
    v_scale,
    spatial,
    spatial_bias,
    w_mix,
    mix_scale,
    ffn_gain,
    w_gate,
    w_up,
    gate_scale,
    up_scale,
    w_down,
    down_scale,
):
    depth, span = w_u.shape
    hidden, out = w_down.shape
    near, far = fold(
        [(depth, 2 * span + w_mix.shape[1]), (3 * hidden, out)],
        mix_gain.reshape(-1, depth),
        w_u,
        w_v,
        w_mix,
        u_scale[None],
        v_scale[None],
        mix_scale,
        ffn_gain.reshape(-1, depth),
        w_gate.T,
        w_up.T,
        w_down,
        down_scale,
    )

    near = lax.all_gather(near, "fs")
    ring = Ring(far)
    steps = ring.count // 2
    pieces = gather_features(tokens)
    early = steps // 2
    for _ in range(early):
        ring.advance()
    pieces[0], *_ = lax.optimization_barrier((pieces[0], *ring.held[-2:]))
    mine, theirs = gating(pieces, near, spatial[0], spatial_bias)
    ring.advance()
    pair = chip_sums(mine, theirs)
    ring.after(*pair[1:])
    ring.advance()
    resid = (tokens.astype(jnp.float32) + sum_chips(pair)).astype(jnp.bfloat16)
    ring.after(resid)
    while ring.step < steps:
        ring.advance()
    mine, theirs = channel(gather_features(resid), gate_scale, up_scale, ring.held)
    pair = chip_sums(mine, theirs)
    return (resid.astype(jnp.float32) + sum_chips(pair)).astype(jnp.bfloat16)


def solution(mesh):
    placed = (
        P(("grp", "fs"), "tp"),
        P(),
        P("fs", "tp"),
        P("fs", "tp"),
        P("tp"),
        P("tp"),
        P("tp", None, None),
        P("tp", None),
        P("tp", "fs"),
        P(None, "fs"),
        P(),
        P("fs", "tp"),
        P("fs", "tp"),
        P("tp"),
        P("tp"),
        P("tp", "fs"),
        P(None, "fs"),
    )
    return jax.shard_map(
        local, mesh=mesh, in_specs=placed, out_specs=P(("grp", "fs"), "tp"), check_vma=False
    )
```

```python
import functools

import jax
import jax.numpy as jnp
from jax import lax
from jax.experimental import pallas as pl
from jax.experimental.pallas import tpu as pltpu
from jax.sharding import PartitionSpec as P

eps = 1e-06
CORES = 2


def swap_cores(x):
    count = lax.axis_size("tp")
    return lax.ppermute(x, "tp", [(i, i ^ 1) for i in range(count)])


def to_chip(x, step):
    count = lax.axis_size("tp")
    return lax.ppermute(x, "tp", [(i, (i + CORES * step) % count) for i in range(count)])


def gather_features(shard):
    chips = lax.axis_size("tp") // CORES
    got = [to_chip(shard, step) for step in range(1, chips)]
    near = swap_cores(jnp.stack([got[0], got[-1]]))
    swapped = [near[0], *[swap_cores(g) for g in got[1:-1]], near[1]]
    return [shard, swap_cores(shard), *[p for pair in zip(got, swapped) for p in pair]]


def chunk_order(me, count):
    chips = count // CORES
    chip, core = lax.div(me, CORES), lax.rem(me, CORES)
    order = []
    for step in range(chips):
        source = CORES * lax.rem(chip + chips - step, chips)
        order += [source + core, source + 1 - core]
    return order


def chip_sums(mine, theirs):
    other = swap_cores(theirs)
    chips = lax.axis_size("tp") // CORES
    pair = [mine[s].astype(jnp.float32) + other[s].astype(jnp.float32) for s in range(chips)]
    return [pair[0]] + [p.astype(jnp.bfloat16) for p in pair[1:]]


def sum_chips(pair):
    total = pair[0]
    for step, p in enumerate(pair[1:], 1):
        total = total + to_chip(p, step).astype(jnp.float32)
    return total


def dot_f32(a, b, dims=(((1,), (0,)), ((), ()))):
    return lax.dot_general(a, b, dims, preferred_element_type=jnp.float32)


def pass_on(x, step):
    count = lax.axis_size("fs")
    return lax.ppermute(x, "fs", [(i, (i + step) % count) for i in range(count)])


class Ring:
    def __init__(self, shard):
        self.count = lax.axis_size("fs")
        self.ahead = self.behind = shard
        self.held = [shard]
        self.before = [shard, shard]
        self.step = 0

    def after(self, *others):
        self.ahead, *_ = lax.optimization_barrier((self.ahead, *others))

    def advance(self):
        self.step += 1
        before, self.before = self.before, [self.ahead, self.behind]
        self.ahead, _ = lax.optimization_barrier((self.ahead, before[1]))
        self.behind, _ = lax.optimization_barrier((self.behind, before[0]))
        self.ahead = pass_on(self.ahead, 1)
        new = [self.ahead]
        if 2 * self.step < self.count:
            self.behind = pass_on(self.behind, -1)
            new.append(self.behind)
        self.held += new
        return new


def ring_order(me, count):
    order = [me]
    for step in range(1, count // 2 + 1):
        order.append(lax.rem(me + count - step, count))
        if 2 * step < count:
            order.append(lax.rem(me + step, count))
    return order


def swap_groups(x):
    count = lax.axis_size("grp")
    return lax.ppermute(x, "grp", [(i, i ^ 1) for i in range(count)])


def lane_block(index, width):
    return pl.ds(pl.multiple_of(index * width, width), width)


def copy_all(pairs, sems, base):
    copies = [
        pltpu.make_async_copy(source, target, sems.at[base + i])
        for i, (source, target) in enumerate(pairs)
    ]
    for copy in copies:
        copy.start()

    def wait():
        for copy in copies:
            copy.wait()

    return wait, base + len(copies)


def load_rows(xs, buf, sems, base):
    width = xs[0].shape[1]
    places = chunk_order(lax.axis_index("tp"), len(xs))
    return copy_all(
        [(x, buf.at[:, lane_block(place, width)]) for x, place in zip(xs, places)], sems, base
    )


def row_factor(x):
    wide = x.astype(jnp.float32)
    return lax.rsqrt(jnp.mean(wide * wide, axis=1, keepdims=True) + eps)


def store_shares(value, weights, chunks, rows, mine_ref, theirs_ref, unroll=False):
    width = mine_ref.shape[2]
    chips = chunks // CORES
    me = lax.axis_index("tp")
    chip, core = lax.div(me, CORES), lax.rem(me, CORES)

    def fill(ref, which):
        def share(step, carry):
            target = CORES * lax.rem(chip + step, chips) + which
            w = weights(lane_block(target, width))
            ref[step, rows, :] = dot_f32(value, w).astype(jnp.bfloat16)
            return carry

        lax.fori_loop(0, chips, share, 0, unroll=unroll)

    fill(mine_ref, core)
    fill(theirs_ref, 1 - core)


def gating_kernel(*refs, chunks, shards, tall):
    xs, refs = refs[:chunks], refs[chunks:]
    near_ref, spatial_ref, bias_ref, mine_ref, theirs_ref, x_buf, in_buf, out_buf, sems = refs
    span = spatial_ref.shape[0]
    lanes = near_ref.shape[2] - 2 * span
    x_here, at = load_rows(xs, x_buf, sems, 0)
    in_here, at = copy_all([(near_ref.at[:, :, : 2 * span], in_buf)], sems, at)
    out_here, at = copy_all(
        [
            (near_ref.at[z, :, 2 * span :], out_buf.at[:, z * lanes : (z + 1) * lanes])
            for z in range(shards)
        ],
        sems,
        at,
    )
    later = lax.broadcasted_iota(jnp.int32, (span, span), 0)
    earlier = lax.broadcasted_iota(jnp.int32, (span, span), 1)
    bias = jnp.broadcast_to(bias_ref[...], (span, span)).T
    mixing = spatial_ref[...]
    mixing = jnp.where(later >= earlier, mixing, jnp.zeros_like(mixing))
    x_here()
    in_here()
    out_here()

    def block(i, carry):
        rows = pl.ds(pl.multiple_of(i * tall, tall), tall)
        x = x_buf[rows, :]
        weights = in_buf[...].reshape(x.shape[1], 2 * span)
        pre = dot_f32(x, weights) * row_factor(x)
        act = 0.5 * pre * (1.0 + lax.erf(pre * (0.5**0.5)))
        u = act[:, :span]
        v = act[:, span:].astype(jnp.bfloat16)
        gated = []
        for b in range(tall // span):
            at = slice(b * span, (b + 1) * span)
            placed = dot_f32(mixing, v[at]) + bias
            gated.append((u[at] * placed).astype(jnp.bfloat16))
        gated = jnp.concatenate(gated, axis=0)
        store_shares(gated, lambda at: out_buf[:, at], chunks, rows, mine_ref, theirs_ref)
        return carry

    lax.fori_loop(0, xs[0].shape[0] // tall, block, 0)


def channel_kernel(*refs, chunks, shards, tall):
    xs, refs = refs[:chunks], refs[chunks:]
    gate_scale_ref, up_scale_ref, refs = *refs[:2], refs[2:]
    ring, refs = refs[:shards], refs[shards:]
    others, refs = refs[:-7], refs[-7:]
    mine_ref, theirs_ref, x_buf, first_buf, down_buf, wide_buf, sems = refs
    lanes = ring[0].shape[1]
    hidden = down_buf.shape[0]
    side = lax.rem(lax.axis_index("grp"), 2)
    around = ring_order(lax.axis_index("fs"), shards)
    parts = [(o, at) for o in others for at in range(0, o.shape[0], hidden)]
    own_buf, other_buf = first_buf.at[side], first_buf.at[1 - side]

    def load(pieces, buf, base):
        return copy_all(
            [
                (w.at[at : at + hidden, :], buf.at[:, lane_block(z, lanes)])
                for z, (w, at) in zip(around, pieces)
            ],
            sems,
            base,
        )

    x_here, at = load_rows(xs, x_buf, sems, 0)
    own_here, at = load([(w, 0) for w in ring], own_buf, at)
    other_here, at = load(parts, other_buf, at)
    down_here, at = load([(w, hidden) for w in ring], down_buf, at)
    across = (((1,), (1,)), ((), ()))
    blocks = xs[0].shape[0] // tall
    x_here()
    own_here()

    def project(step, carry):
        which = lax.select(step == 0, side, 1 - side)
        pl.when(step == 1)(other_here)

        def block(i, carry):
            rows = pl.ds(pl.multiple_of(i * tall, tall), tall)
            wide_buf[which, rows, :] = dot_f32(x_buf[rows, :], first_buf[which], across)
            return carry

        return lax.fori_loop(0, blocks, block, carry)

    lax.fori_loop(0, 2, project, 0)
    down_here()

    def block(i, carry):
        rows = pl.ds(pl.multiple_of(i * tall, tall), tall)
        factor = row_factor(x_buf[rows, :])
        gate = wide_buf[0, rows, :] * factor * gate_scale_ref[...][None, :]
        up = wide_buf[1, rows, :] * factor * up_scale_ref[...][None, :]
        act = (gate / (1.0 + jnp.exp(-gate)) * up).astype(jnp.bfloat16)
        store_shares(act, lambda at: down_buf[:, at], chunks, rows, mine_ref, theirs_ref, True)
        return carry

    lax.fori_loop(0, blocks, block, 0)


def gain_rows(gain_ref):
    row = gain_ref[pl.ds(lax.axis_index("fs"), 1), :]
    return jnp.broadcast_to(row, (row.shape[1], row.shape[1]))


def fold_kernel(
    in_gain_ref,
    u_ref,
    v_ref,
    mix_ref,
    u_scale_ref,
    v_scale_ref,
    mix_scale_ref,
    mid_gain_ref,
    gate_ref,
    up_ref,
    down_ref,
    down_scale_ref,
    near_ref,
    far_ref,
    other_ref,
):
    gain = gain_rows(in_gain_ref).T
    parts = [
        u_ref[...] * gain * u_scale_ref[...],
        v_ref[...] * gain * v_scale_ref[...],
        mix_ref[...] * mix_scale_ref[...],
    ]
    at = 0
    for part in parts:
        near_ref[:, at : at + part.shape[1]] = part.astype(jnp.bfloat16)
        at += part.shape[1]
    gain = gain_rows(mid_gain_ref)[:1, :]
    hidden = gate_ref.shape[0]
    even = lax.rem(lax.axis_index("grp"), 2) == 0
    gate, up = gate_ref[...], up_ref[...]
    far_ref[:hidden, :] = (jnp.where(even, gate, up) * gain).astype(jnp.bfloat16)
    far_ref[hidden:, :] = (down_ref[...] * down_scale_ref[...]).astype(jnp.bfloat16)
    other_ref[...] = (jnp.where(even, up, gate) * gain).astype(jnp.bfloat16)


def fold(shapes, *operands):
    return pl.pallas_call(
        fold_kernel,
        grid=(1,),
        in_specs=[pl.BlockSpec(a.shape, lambda i: (0, 0)) for a in operands],
        out_specs=[pl.BlockSpec(memory_space=pltpu.VMEM)] * len(shapes),
        out_shape=[jax.ShapeDtypeStruct(shape, jnp.bfloat16) for shape in shapes],
        cost_estimate=pl.CostEstimate(flops=2**22, bytes_accessed=2**20, transcendentals=0),
        compiler_params=pltpu.CompilerParams(vmem_limit_bytes=60 * 2**20),
        name="fold",
    )(*operands)


def call(kernel, name, operands, specs, chunks, shards, tall, scratch, flops, limit):
    rows, width = operands[0].shape
    half = chunks // CORES
    vmem = pl.BlockSpec(memory_space=pltpu.VMEM)
    return pl.pallas_call(
        functools.partial(kernel, chunks=chunks, shards=shards, tall=tall),
        in_specs=[vmem if spec is None else spec for spec in specs],
        out_specs=[vmem, vmem],
        out_shape=[jax.ShapeDtypeStruct((half, rows, width), jnp.bfloat16)] * 2,
        scratch_shapes=[
            pltpu.VMEM(shape, jnp.bfloat16) if isinstance(shape, tuple) else shape
            for shape in scratch
        ],
        compiler_params=pltpu.CompilerParams(vmem_limit_bytes=limit * 2**20),
        cost_estimate=pl.CostEstimate(flops=flops, bytes_accessed=2**20, transcendentals=0),
        name=name,
    )(*operands)


def gating(pieces, near, spatial, bias):
    chunks, shards, tall = len(pieces), near.shape[0], 256
    rows, width = pieces[0].shape
    span = spatial.shape[0]
    model = chunks * width
    flops = 2 * rows * (model * 2 * span + span * span + span * model)
    scratch = [
        (rows, model),
        (shards, model // shards, 2 * span),
        (span, model),
        pltpu.SemaphoreType.DMA((chunks + 1 + shards,)),
    ]
    operands = [*pieces, near, spatial, bias]
    specs = [pl.BlockSpec(memory_space=pl.ANY)] * (chunks + 1) + [None] * 2
    return call(gating_kernel, "gating", operands, specs, chunks, shards, tall, scratch, flops, 16)


def channel(pieces, gate_scale, up_scale, ring, others):
    chunks, shards, tall = len(pieces), len(ring), 256
    rows, width = pieces[0].shape
    hidden = gate_scale.shape[0]
    model = chunks * width
    flops = 2 * rows * model * 3 * hidden
    scratch = [
        (rows, model),
        (2, hidden, model),
        (hidden, model),
        pltpu.VMEM((2, rows, hidden), jnp.float32),
        pltpu.SemaphoreType.DMA((chunks + 3 * shards,)),
    ]
    operands = [*pieces, gate_scale, up_scale, *ring, *others]
    specs = [pl.BlockSpec(memory_space=pl.ANY)] * len(operands)
    specs[chunks] = specs[chunks + 1] = None
    return call(channel_kernel, "channel", operands, specs, chunks, shards, tall, scratch, flops, 57)


def local(
    tokens,
    mix_gain,
    w_u,
    w_v,
    u_scale,
    v_scale,
    spatial,
    spatial_bias,
    w_mix,
    mix_scale,
    ffn_gain,
    w_gate,
    w_up,
    gate_scale,
    up_scale,
    w_down,
    down_scale,
):
    depth, span = w_u.shape
    hidden, out = w_down.shape
    near, far, other = fold(
        [(depth, 2 * span + w_mix.shape[1]), (2 * hidden, out), (hidden, depth)],
        mix_gain.reshape(-1, depth),
        w_u,
        w_v,
        w_mix,
        u_scale[None],
        v_scale[None],
        mix_scale,
        ffn_gain.reshape(-1, depth),
        w_gate.T,
        w_up.T,
        w_down,
        down_scale,
    )

    near = lax.all_gather(near, "fs")
    ring = Ring(far)
    steps = ring.count // 2
    pieces = gather_features(tokens)
    others = [other]

    def two_rounds():
        new = []
        for _ in range(2):
            if ring.step < steps:
                new += ring.advance()
        swapped = swap_groups(jnp.concatenate([piece[:hidden] for piece in new], axis=0))
        others.append(swapped)

    two_rounds()
    two_rounds()
    pieces[0], *_ = lax.optimization_barrier((pieces[0], *ring.held[-2:], others[1]))
    mine, theirs = gating(pieces, near, spatial[0], spatial_bias)
    two_rounds()
    pair = chip_sums(mine, theirs)
    resid = (tokens.astype(jnp.float32) + sum_chips(pair)).astype(jnp.bfloat16)
    ring.after(others[2], *pair[1:])
    while ring.step < steps:
        two_rounds()
    mine, theirs = channel(gather_features(resid), gate_scale, up_scale, ring.held, others)
    pair = chip_sums(mine, theirs)
    return (resid.astype(jnp.float32) + sum_chips(pair)).astype(jnp.bfloat16)


def solution(mesh):
    placed = (
        P(("grp", "fs"), "tp"),
        P(),
        P("fs", "tp"),
        P("fs", "tp"),
        P("tp"),
        P("tp"),
        P("tp", None, None),
        P("tp", None),
        P("tp", "fs"),
        P(None, "fs"),
        P(),
        P("fs", "tp"),
        P("fs", "tp"),
        P("tp"),
        P("tp"),
        P("tp", "fs"),
        P(None, "fs"),
    )
    return jax.shard_map(
        local, mesh=mesh, in_specs=placed, out_specs=P(("grp", "fs"), "tp"), check_vma=False
    )
```

```python
import functools

import jax
import jax.numpy as jnp
from jax import lax
from jax.experimental import pallas as pl
from jax.experimental.pallas import tpu as pltpu
from jax.sharding import PartitionSpec as P

eps = 1e-06
CORES = 2


def swap_cores(x):
    count = lax.axis_size("tp")
    return lax.ppermute(x, "tp", [(i, i ^ 1) for i in range(count)])


def to_chip(x, step):
    count = lax.axis_size("tp")
    return lax.ppermute(x, "tp", [(i, (i + CORES * step) % count) for i in range(count)])


def gather_features(shard, together=False):
    chips = lax.axis_size("tp") // CORES
    got = [shard]
    got += [to_chip(shard, step) for step in range(1, chips)]
    if together:
        other = swap_cores(jnp.stack(got[1:]))
        swapped = [swap_cores(shard), *[other[i] for i in range(chips - 1)]]
    else:
        swapped = [swap_cores(g) for g in got]
    return [piece for pair in zip(got, swapped) for piece in pair]


def chunk_order(me, count):
    chips = count // CORES
    chip, core = lax.div(me, CORES), lax.rem(me, CORES)
    order = []
    for step in range(chips):
        source = CORES * lax.rem(chip + chips - step, chips)
        order += [source + core, source + 1 - core]
    return order


def chip_sums(mine, theirs):
    other = swap_cores(theirs)
    chips = lax.axis_size("tp") // CORES
    pair = [mine[s].astype(jnp.float32) + other[s].astype(jnp.float32) for s in range(chips)]
    return [pair[0]] + [p.astype(jnp.bfloat16) for p in pair[1:]]


def sum_chips(pair):
    total = pair[0]
    for step, p in enumerate(pair[1:], 1):
        total = total + to_chip(p, step).astype(jnp.float32)
    return total


def dot_f32(a, b, dims=(((1,), (0,)), ((), ()))):
    return lax.dot_general(a, b, dims, preferred_element_type=jnp.float32)


def pass_on(x, step):
    count = lax.axis_size("fs")
    return lax.ppermute(x, "fs", [(i, (i + step) % count) for i in range(count)])


class Ring:
    def __init__(self, shard):
        self.count = lax.axis_size("fs")
        self.ahead = self.behind = shard
        self.held = [shard]
        self.before = [shard, shard]
        self.step = 0

    def advance(self):
        self.step += 1
        before, self.before = self.before, [self.ahead, self.behind]
        self.ahead, _ = lax.optimization_barrier((self.ahead, before[1]))
        self.behind, _ = lax.optimization_barrier((self.behind, before[0]))
        self.ahead = pass_on(self.ahead, 1)
        new = [self.ahead]
        if 2 * self.step < self.count:
            self.behind = pass_on(self.behind, -1)
            new.append(self.behind)
        self.held += new
        return new


def ring_order(me, count):
    order = [me]
    for step in range(1, count // 2 + 1):
        order.append(lax.rem(me + count - step, count))
        if 2 * step < count:
            order.append(lax.rem(me + step, count))
    return order


def lane_block(index, width):
    return pl.ds(pl.multiple_of(index * width, width), width)


def copy_all(pairs, sems, base):
    copies = [
        pltpu.make_async_copy(source, target, sems.at[base + i])
        for i, (source, target) in enumerate(pairs)
    ]
    for copy in copies:
        copy.start()

    def wait():
        for copy in copies:
            copy.wait()

    return wait, base + len(copies)


def load_rows(xs, buf, sems, base):
    width = xs[0].shape[1]
    places = chunk_order(lax.axis_index("tp"), len(xs))
    return copy_all(
        [(x, buf.at[:, lane_block(place, width)]) for x, place in zip(xs, places)], sems, base
    )


def row_factor(x):
    wide = x.astype(jnp.float32)
    return lax.rsqrt(jnp.mean(wide * wide, axis=1, keepdims=True) + eps)


def store_shares(value, weights, chunks, rows, mine_ref, theirs_ref, unroll=False):
    width = mine_ref.shape[2]
    chips = chunks // CORES
    me = lax.axis_index("tp")
    chip, core = lax.div(me, CORES), lax.rem(me, CORES)

    def fill(ref, which):
        def share(step, carry):
            target = CORES * lax.rem(chip + step, chips) + which
            w = weights(lane_block(target, width))
            ref[step, rows, :] = dot_f32(value, w).astype(jnp.bfloat16)
            return carry

        lax.fori_loop(0, chips, share, 0, unroll=unroll)

    fill(mine_ref, core)
    fill(theirs_ref, 1 - core)


def take_rows(xs, places, rows, buf):
    width = xs[0].shape[1]
    squares = None
    for place, x_ref in zip(places, xs):
        x = x_ref[rows, :]
        buf[:, lane_block(place, width)] = x
        wide = x.astype(jnp.float32)
        sq = jnp.sum(wide * wide, axis=1, keepdims=True)
        squares = sq if squares is None else squares + sq
    return lax.rsqrt(squares * (1.0 / (len(xs) * width)) + eps)


def gating_kernel(*refs, chunks, shards, tall):
    xs, ws = refs[:chunks], refs[chunks : chunks + shards]
    spatial_ref, bias_ref, mine_ref, theirs_ref, x_buf, in_buf, out_buf = refs[chunks + shards :]
    span = spatial_ref.shape[0]
    depth = ws[0].shape[0]
    sources = chunk_order(lax.axis_index("tp"), chunks)
    for z, w in zip(ring_order(lax.axis_index("fs"), shards), ws):
        in_buf[lane_block(z, depth), :] = w[:, : 2 * span]
        out_buf[:, lane_block(z, w.shape[1] - 2 * span)] = w[:, 2 * span :]
    later = lax.broadcasted_iota(jnp.int32, (span, span), 0)
    earlier = lax.broadcasted_iota(jnp.int32, (span, span), 1)
    bias = jnp.broadcast_to(bias_ref[...], (span, span)).T
    mixing = spatial_ref[...]
    mixing = jnp.where(later >= earlier, mixing, jnp.zeros_like(mixing))

    def block(i, carry):
        rows = pl.ds(pl.multiple_of(i * tall, tall), tall)
        factor = take_rows(xs, sources, rows, x_buf)
        pre = dot_f32(x_buf[...], in_buf[...]) * factor
        act = 0.5 * pre * (1.0 + lax.erf(pre * (0.5**0.5)))
        u = act[:, :span]
        v = act[:, span:].astype(jnp.bfloat16)
        gated = []
        for b in range(tall // span):
            at = slice(b * span, (b + 1) * span)
            placed = dot_f32(mixing, v[at]) + bias
            gated.append((u[at] * placed).astype(jnp.bfloat16))
        gated = jnp.concatenate(gated, axis=0)
        store_shares(gated, lambda at: out_buf[:, at], chunks, rows, mine_ref, theirs_ref)
        return carry

    lax.fori_loop(0, xs[0].shape[0] // tall, block, 0)


def channel_kernel(*refs, chunks, shards, tall):
    xs, refs = refs[:chunks], refs[chunks:]
    gate_scale_ref, up_scale_ref, far_ref, mine_ref, theirs_ref = refs[:5]
    x_buf, first_buf, down_buf, wide_buf, sems = refs[5:]
    lanes = far_ref.shape[2]
    hidden = down_buf.shape[0]

    def load(part, buf, base):
        rows = slice(part * hidden, (part + 1) * hidden)
        return copy_all(
            [
                (far_ref.at[z, rows, :], buf.at[:, z * lanes : (z + 1) * lanes])
                for z in range(shards)
            ],
            sems,
            base,
        )

    x_here, at = load_rows(xs, x_buf, sems, 0)
    gate_here, at = load(0, first_buf.at[0], at)
    up_here, at = load(1, first_buf.at[1], at)
    down_here, at = load(2, down_buf, at)
    across = (((1,), (1,)), ((), ()))
    blocks = xs[0].shape[0] // tall
    x_here()
    gate_here()

    def project(step, carry):
        pl.when(step == 1)(up_here)

        def block(i, carry):
            rows = pl.ds(pl.multiple_of(i * tall, tall), tall)
            wide_buf[step, rows, :] = dot_f32(x_buf[rows, :], first_buf[step], across)
            return carry

        return lax.fori_loop(0, blocks, block, carry)

    lax.fori_loop(0, 2, project, 0)
    down_here()

    def block(i, carry):
        rows = pl.ds(pl.multiple_of(i * tall, tall), tall)
        factor = row_factor(x_buf[rows, :])
        gate = wide_buf[0, rows, :] * factor * gate_scale_ref[...][None, :]
        up = wide_buf[1, rows, :] * factor * up_scale_ref[...][None, :]
        act = (gate / (1.0 + jnp.exp(-gate)) * up).astype(jnp.bfloat16)
        store_shares(act, lambda at: down_buf[:, at], chunks, rows, mine_ref, theirs_ref, True)
        return carry

    lax.fori_loop(0, blocks, block, 0)


def gain_rows(gain_ref):
    row = gain_ref[pl.ds(lax.axis_index("fs"), 1), :]
    return jnp.broadcast_to(row, (row.shape[1], row.shape[1]))


def fold_kernel(
    in_gain_ref,
    u_ref,
    v_ref,
    mix_ref,
    u_scale_ref,
    v_scale_ref,
    mix_scale_ref,
    mid_gain_ref,
    gate_ref,
    up_ref,
    down_ref,
    down_scale_ref,
    near_ref,
    far_ref,
):
    gain = gain_rows(in_gain_ref).T
    parts = [
        u_ref[...] * gain * u_scale_ref[...],
        v_ref[...] * gain * v_scale_ref[...],
        mix_ref[...] * mix_scale_ref[...],
    ]
    at = 0
    for part in parts:
        near_ref[:, at : at + part.shape[1]] = part.astype(jnp.bfloat16)
        at += part.shape[1]
    gain = gain_rows(mid_gain_ref)[:1, :]
    hidden = gate_ref.shape[0]
    far_ref[:hidden, :] = (gate_ref[...] * gain).astype(jnp.bfloat16)
    far_ref[hidden : 2 * hidden, :] = (up_ref[...] * gain).astype(jnp.bfloat16)
    far_ref[2 * hidden :, :] = (down_ref[...] * down_scale_ref[...]).astype(jnp.bfloat16)


def fold(shapes, *operands):
    return pl.pallas_call(
        fold_kernel,
        grid=(1,),
        in_specs=[pl.BlockSpec(a.shape, lambda i: (0, 0)) for a in operands],
        out_specs=[pl.BlockSpec(memory_space=pltpu.VMEM)] * len(shapes),
        out_shape=[jax.ShapeDtypeStruct(shape, jnp.bfloat16) for shape in shapes],
        cost_estimate=pl.CostEstimate(flops=2**22, bytes_accessed=2**20, transcendentals=0),
        compiler_params=pltpu.CompilerParams(vmem_limit_bytes=60 * 2**20),
        name="fold",
    )(*operands)


def call(kernel, name, operands, specs, chunks, shards, tall, scratch, flops, limit):
    rows, width = operands[0].shape
    half = chunks // CORES
    vmem = pl.BlockSpec(memory_space=pltpu.VMEM)
    return pl.pallas_call(
        functools.partial(kernel, chunks=chunks, shards=shards, tall=tall),
        in_specs=[vmem if spec is None else spec for spec in specs],
        out_specs=[vmem, vmem],
        out_shape=[jax.ShapeDtypeStruct((half, rows, width), jnp.bfloat16)] * 2,
        scratch_shapes=[
            pltpu.VMEM(shape, jnp.bfloat16) if isinstance(shape, tuple) else shape
            for shape in scratch
        ],
        compiler_params=pltpu.CompilerParams(vmem_limit_bytes=limit * 2**20),
        cost_estimate=pl.CostEstimate(flops=flops, bytes_accessed=2**20, transcendentals=0),
        name=name,
    )(*operands)


def gating(pieces, weights, spatial, bias):
    chunks, shards, tall = len(pieces), len(weights), 256
    rows, width = pieces[0].shape
    span = spatial.shape[0]
    model = chunks * width
    flops = 2 * rows * (model * 2 * span + span * span + span * model)
    scratch = [(tall, model), (model, 2 * span), (span, model)]
    operands = [*pieces, *weights, spatial, bias]
    specs = [None] * len(operands)
    return call(gating_kernel, "gating", operands, specs, chunks, shards, tall, scratch, flops, 16)


def channel(pieces, gate_scale, up_scale, far):
    chunks, shards, tall = len(pieces), far.shape[0], 256
    rows, width = pieces[0].shape
    hidden = gate_scale.shape[0]
    model = chunks * width
    flops = 2 * rows * model * 3 * hidden
    scratch = [
        (rows, model),
        (2, hidden, model),
        (hidden, model),
        pltpu.VMEM((2, rows, hidden), jnp.float32),
        pltpu.SemaphoreType.DMA((chunks + 3 * shards,)),
    ]
    operands = [*pieces, gate_scale, up_scale, far]
    specs = [pl.BlockSpec(memory_space=pl.ANY)] * len(operands)
    specs[chunks] = specs[chunks + 1] = None
    return call(channel_kernel, "channel", operands, specs, chunks, shards, tall, scratch, flops, 57)


def local(
    tokens,
    mix_gain,
    w_u,
    w_v,
    u_scale,
    v_scale,
    spatial,
    spatial_bias,
    w_mix,
    mix_scale,
    ffn_gain,
    w_gate,
    w_up,
    gate_scale,
    up_scale,
    w_down,
    down_scale,
):
    depth, span = w_u.shape
    hidden, out = w_down.shape
    near, far = fold(
        [(depth, 2 * span + w_mix.shape[1]), (3 * hidden, out)],
        mix_gain.reshape(-1, depth),
        w_u,
        w_v,
        w_mix,
        u_scale[None],
        v_scale[None],
        mix_scale,
        ffn_gain.reshape(-1, depth),
        w_gate.T,
        w_up.T,
        w_down,
        down_scale,
    )

    far = lax.all_gather(far, "fs")
    ring = Ring(near)
    for _ in range(ring.count // 2):
        ring.advance()
    mine, theirs = gating(gather_features(tokens, True), ring.held, spatial[0], spatial_bias)
    resid = (tokens.astype(jnp.float32) + sum_chips(chip_sums(mine, theirs))).astype(jnp.bfloat16)
    mine, theirs = channel(gather_features(resid), gate_scale, up_scale, far)
    pair = chip_sums(mine, theirs)
    return (resid.astype(jnp.float32) + sum_chips(pair)).astype(jnp.bfloat16)


def solution(mesh):
    placed = (
        P(("grp", "fs"), "tp"),
        P(),
        P("fs", "tp"),
        P("fs", "tp"),
        P("tp"),
        P("tp"),
        P("tp", None, None),
        P("tp", None),
        P("tp", "fs"),
        P(None, "fs"),
        P(),
        P("fs", "tp"),
        P("fs", "tp"),
        P("tp"),
        P("tp"),
        P("tp", "fs"),
        P(None, "fs"),
    )
    return jax.shard_map(
        local, mesh=mesh, in_specs=placed, out_specs=P(("grp", "fs"), "tp"), check_vma=False
    )
```

```python
import functools

import jax
import jax.numpy as jnp
from jax import lax
from jax.experimental import pallas as pl
from jax.experimental.pallas import tpu as pltpu
from jax.sharding import PartitionSpec as P

eps = 1e-06
CORES = 2


def swap_cores(x):
    count = lax.axis_size("tp")
    return lax.ppermute(x, "tp", [(i, i ^ 1) for i in range(count)])


def to_chip(x, step):
    count = lax.axis_size("tp")
    return lax.ppermute(x, "tp", [(i, (i + CORES * step) % count) for i in range(count)])


def from_chips(shard):
    chips = lax.axis_size("tp") // CORES
    return [to_chip(shard, step) for step in range(1, chips)]


def gather_features(shard):
    got = [shard, *from_chips(shard)]
    return [piece for g in got for piece in (g, swap_cores(g))]


def chunk_order(me, count):
    chips = count // CORES
    chip, core = lax.div(me, CORES), lax.rem(me, CORES)
    order = []
    for step in range(chips):
        source = CORES * lax.rem(chip + chips - step, chips)
        order += [source + core, source + 1 - core]
    return order


def chip_sums(mine, theirs):
    other = swap_cores(theirs)
    chips = lax.axis_size("tp") // CORES
    pair = [mine[s].astype(jnp.float32) + other[s].astype(jnp.float32) for s in range(chips)]
    return [pair[0]] + [p.astype(jnp.bfloat16) for p in pair[1:]]


def sum_chips(pair):
    total = pair[0]
    for step, p in enumerate(pair[1:], 1):
        total = total + to_chip(p, step).astype(jnp.float32)
    return total


def dot_f32(a, b, dims=(((1,), (0,)), ((), ()))):
    return lax.dot_general(a, b, dims, preferred_element_type=jnp.float32)


def pass_on(x, step):
    count = lax.axis_size("fs")
    return lax.ppermute(x, "fs", [(i, (i + step) % count) for i in range(count)])


class Ring:
    def __init__(self, shard):
        self.count = lax.axis_size("fs")
        self.ahead = self.behind = shard
        self.held = [shard]
        self.before = [shard, shard]
        self.step = 0

    def advance(self):
        self.step += 1
        before, self.before = self.before, [self.ahead, self.behind]
        self.ahead, _ = lax.optimization_barrier((self.ahead, before[1]))
        self.behind, _ = lax.optimization_barrier((self.behind, before[0]))
        self.ahead = pass_on(self.ahead, 1)
        new = [self.ahead]
        if 2 * self.step < self.count:
            self.behind = pass_on(self.behind, -1)
            new.append(self.behind)
        self.held += new
        return new


def ring_order(me, count):
    order = [me]
    for step in range(1, count // 2 + 1):
        order.append(lax.rem(me + count - step, count))
        if 2 * step < count:
            order.append(lax.rem(me + step, count))
    return order


def lane_block(index, width):
    return pl.ds(pl.multiple_of(index * width, width), width)


def copy_all(pairs, sems, base):
    copies = [
        pltpu.make_async_copy(source, target, sems.at[base + i])
        for i, (source, target) in enumerate(pairs)
    ]
    for copy in copies:
        copy.start()

    def wait():
        for copy in copies:
            copy.wait()

    return wait, base + len(copies)


def load_rows(xs, buf, sems, base):
    width = xs[0].shape[1]
    places = chunk_order(lax.axis_index("tp"), len(xs))
    return copy_all(
        [(x, buf.at[:, lane_block(place, width)]) for x, place in zip(xs, places)], sems, base
    )


def row_factor(x):
    wide = x.astype(jnp.float32)
    return lax.rsqrt(jnp.mean(wide * wide, axis=1, keepdims=True) + eps)


def store_shares(value, weights, chunks, rows, mine_ref, theirs_ref, unroll=False):
    width = mine_ref.shape[2]
    chips = chunks // CORES
    me = lax.axis_index("tp")
    chip, core = lax.div(me, CORES), lax.rem(me, CORES)

    def fill(ref, which):
        def share(step, carry):
            target = CORES * lax.rem(chip + step, chips) + which
            w = weights(lane_block(target, width))
            ref[step, rows, :] = dot_f32(value, w).astype(jnp.bfloat16)
            return carry

        lax.fori_loop(0, chips, share, 0, unroll=unroll)

    fill(mine_ref, core)
    fill(theirs_ref, 1 - core)


def take_rows(xs, places, rows, buf):
    width = xs[0].shape[1]
    squares = None
    for place, x_ref in zip(places, xs):
        x = x_ref[rows, :]
        buf[:, lane_block(place, width)] = x
        wide = x.astype(jnp.float32)
        sq = jnp.sum(wide * wide, axis=1, keepdims=True)
        squares = sq if squares is None else squares + sq
    return lax.rsqrt(squares * (1.0 / (len(xs) * width)) + eps)


def gating_kernel(*refs, chunks, shards, tall):
    xs, ws = refs[:chunks], refs[chunks : chunks + shards]
    spatial_ref, bias_ref, mine_ref, theirs_ref, x_buf, in_buf, out_buf = refs[chunks + shards :]
    span = spatial_ref.shape[0]
    depth = ws[0].shape[0]
    sources = chunk_order(lax.axis_index("tp"), chunks)
    for z, w in zip(ring_order(lax.axis_index("fs"), shards), ws):
        in_buf[lane_block(z, depth), :] = w[:, : 2 * span]
        out_buf[:, lane_block(z, w.shape[1] - 2 * span)] = w[:, 2 * span :]
    later = lax.broadcasted_iota(jnp.int32, (span, span), 0)
    earlier = lax.broadcasted_iota(jnp.int32, (span, span), 1)
    bias = jnp.broadcast_to(bias_ref[...], (span, span)).T
    mixing = spatial_ref[...]
    mixing = jnp.where(later >= earlier, mixing, jnp.zeros_like(mixing))

    def block(i, carry):
        rows = pl.ds(pl.multiple_of(i * tall, tall), tall)
        factor = take_rows(xs, sources, rows, x_buf)
        pre = dot_f32(x_buf[...], in_buf[...]) * factor
        act = 0.5 * pre * (1.0 + lax.erf(pre * (0.5**0.5)))
        u = act[:, :span]
        v = act[:, span:].astype(jnp.bfloat16)
        gated = []
        for b in range(tall // span):
            at = slice(b * span, (b + 1) * span)
            placed = dot_f32(mixing, v[at]) + bias
            gated.append((u[at] * placed).astype(jnp.bfloat16))
        gated = jnp.concatenate(gated, axis=0)
        store_shares(gated, lambda at: out_buf[:, at], chunks, rows, mine_ref, theirs_ref)
        return carry

    lax.fori_loop(0, xs[0].shape[0] // tall, block, 0)


def channel_kernel(*refs, chunks, shards, tall):
    xs, refs = refs[:chunks], refs[chunks:]
    gate_scale_ref, up_scale_ref, far_ref, mine_ref, theirs_ref = refs[:5]
    x_buf, first_buf, down_buf, wide_buf, sems = refs[5:]
    lanes = far_ref.shape[2]
    hidden = down_buf.shape[0]

    def load(part, buf, base):
        rows = slice(part * hidden, (part + 1) * hidden)
        return copy_all(
            [
                (far_ref.at[z, rows, :], buf.at[:, z * lanes : (z + 1) * lanes])
                for z in range(shards)
            ],
            sems,
            base,
        )

    x_here, at = load_rows(xs, x_buf, sems, 0)
    gate_here, at = load(0, first_buf.at[0], at)
    up_here, at = load(1, first_buf.at[1], at)
    down_here, at = load(2, down_buf, at)
    across = (((1,), (1,)), ((), ()))
    blocks = xs[0].shape[0] // tall
    x_here()
    gate_here()

    def project(step, carry):
        pl.when(step == 1)(up_here)

        def block(i, carry):
            rows = pl.ds(pl.multiple_of(i * tall, tall), tall)
            wide_buf[step, rows, :] = dot_f32(x_buf[rows, :], first_buf[step], across)
            return carry

        return lax.fori_loop(0, blocks, block, carry)

    lax.fori_loop(0, 2, project, 0)
    down_here()

    def block(i, carry):
        rows = pl.ds(pl.multiple_of(i * tall, tall), tall)
        factor = row_factor(x_buf[rows, :])
        gate = wide_buf[0, rows, :] * factor * gate_scale_ref[...][None, :]
        up = wide_buf[1, rows, :] * factor * up_scale_ref[...][None, :]
        act = (gate / (1.0 + jnp.exp(-gate)) * up).astype(jnp.bfloat16)
        store_shares(act, lambda at: down_buf[:, at], chunks, rows, mine_ref, theirs_ref, True)
        return carry

    lax.fori_loop(0, blocks, block, 0)


def gain_rows(gain_ref):
    row = gain_ref[pl.ds(lax.axis_index("fs"), 1), :]
    return jnp.broadcast_to(row, (row.shape[1], row.shape[1]))


def fold_kernel(
    in_gain_ref,
    u_ref,
    v_ref,
    mix_ref,
    u_scale_ref,
    v_scale_ref,
    mix_scale_ref,
    mid_gain_ref,
    gate_ref,
    up_ref,
    down_ref,
    down_scale_ref,
    near_ref,
    far_ref,
):
    gain = gain_rows(in_gain_ref).T
    parts = [
        u_ref[...] * gain * u_scale_ref[...],
        v_ref[...] * gain * v_scale_ref[...],
        mix_ref[...] * mix_scale_ref[...],
    ]
    at = 0
    for part in parts:
        near_ref[:, at : at + part.shape[1]] = part.astype(jnp.bfloat16)
        at += part.shape[1]
    gain = gain_rows(mid_gain_ref)[:1, :]
    hidden = gate_ref.shape[0]
    far_ref[:hidden, :] = (gate_ref[...] * gain).astype(jnp.bfloat16)
    far_ref[hidden : 2 * hidden, :] = (up_ref[...] * gain).astype(jnp.bfloat16)
    far_ref[2 * hidden :, :] = (down_ref[...] * down_scale_ref[...]).astype(jnp.bfloat16)


def fold(shapes, *operands):
    return pl.pallas_call(
        fold_kernel,
        grid=(1,),
        in_specs=[pl.BlockSpec(a.shape, lambda i: (0, 0)) for a in operands],
        out_specs=[pl.BlockSpec(memory_space=pltpu.VMEM)] * len(shapes),
        out_shape=[jax.ShapeDtypeStruct(shape, jnp.bfloat16) for shape in shapes],
        cost_estimate=pl.CostEstimate(flops=2**22, bytes_accessed=2**20, transcendentals=0),
        compiler_params=pltpu.CompilerParams(vmem_limit_bytes=60 * 2**20),
        name="fold",
    )(*operands)


def call(kernel, name, operands, specs, chunks, shards, tall, scratch, flops, limit):
    rows, width = operands[0].shape
    half = chunks // CORES
    vmem = pl.BlockSpec(memory_space=pltpu.VMEM)
    return pl.pallas_call(
        functools.partial(kernel, chunks=chunks, shards=shards, tall=tall),
        in_specs=[vmem if spec is None else spec for spec in specs],
        out_specs=[vmem, vmem],
        out_shape=[jax.ShapeDtypeStruct((half, rows, width), jnp.bfloat16)] * 2,
        scratch_shapes=[
            pltpu.VMEM(shape, jnp.bfloat16) if isinstance(shape, tuple) else shape
            for shape in scratch
        ],
        compiler_params=pltpu.CompilerParams(vmem_limit_bytes=limit * 2**20),
        cost_estimate=pl.CostEstimate(flops=flops, bytes_accessed=2**20, transcendentals=0),
        name=name,
    )(*operands)


def gating(pieces, weights, spatial, bias):
    chunks, shards, tall = len(pieces), len(weights), 256
    rows, width = pieces[0].shape
    span = spatial.shape[0]
    model = chunks * width
    flops = 2 * rows * (model * 2 * span + span * span + span * model)
    scratch = [(tall, model), (model, 2 * span), (span, model)]
    operands = [*pieces, *weights, spatial, bias]
    specs = [None] * len(operands)
    return call(gating_kernel, "gating", operands, specs, chunks, shards, tall, scratch, flops, 16)


def channel(pieces, gate_scale, up_scale, far):
    chunks, shards, tall = len(pieces), far.shape[0], 256
    rows, width = pieces[0].shape
    hidden = gate_scale.shape[0]
    model = chunks * width
    flops = 2 * rows * model * 3 * hidden
    scratch = [
        (rows, model),
        (2, hidden, model),
        (hidden, model),
        pltpu.VMEM((2, rows, hidden), jnp.float32),
        pltpu.SemaphoreType.DMA((chunks + 3 * shards,)),
    ]
    operands = [*pieces, gate_scale, up_scale, far]
    specs = [pl.BlockSpec(memory_space=pl.ANY)] * len(operands)
    specs[chunks] = specs[chunks + 1] = None
    return call(channel_kernel, "channel", operands, specs, chunks, shards, tall, scratch, flops, 50)


def local(
    tokens,
    mix_gain,
    w_u,
    w_v,
    u_scale,
    v_scale,
    spatial,
    spatial_bias,
    w_mix,
    mix_scale,
    ffn_gain,
    w_gate,
    w_up,
    gate_scale,
    up_scale,
    w_down,
    down_scale,
):
    depth, span = w_u.shape
    hidden, out = w_down.shape
    near, far = fold(
        [(depth, 2 * span + w_mix.shape[1]), (3 * hidden, out)],
        mix_gain.reshape(-1, depth),
        w_u,
        w_v,
        w_mix,
        u_scale[None],
        v_scale[None],
        mix_scale,
        ffn_gain.reshape(-1, depth),
        w_gate.T,
        w_up.T,
        w_down,
        down_scale,
    )

    far = lax.all_gather(far, "fs")
    ring = Ring(near)
    steps = ring.count // 2
    ring.advance()
    shard, *_ = lax.optimization_barrier((tokens, *ring.advance()))
    got = from_chips(shard)
    while ring.step < steps - 2:
        ring.advance()
    *got, _, _ = lax.optimization_barrier((*got, *ring.held[-2:]))
    other = swap_cores(jnp.stack(got))
    while ring.step < steps:
        ring.advance()
    pieces = [tokens, swap_cores(shard)]
    for i, piece in enumerate(got):
        pieces += [piece, other[i]]
    mine, theirs = gating(pieces, ring.held, spatial[0], spatial_bias)
    resid = (tokens.astype(jnp.float32) + sum_chips(chip_sums(mine, theirs))).astype(jnp.bfloat16)
    mine, theirs = channel(gather_features(resid), gate_scale, up_scale, far)
    pair = chip_sums(mine, theirs)
    return (resid.astype(jnp.float32) + sum_chips(pair)).astype(jnp.bfloat16)


def solution(mesh):
    placed = (
        P(("grp", "fs"), "tp"),
        P(),
        P("fs", "tp"),
        P("fs", "tp"),
        P("tp"),
        P("tp"),
        P("tp", None, None),
        P("tp", None),
        P("tp", "fs"),
        P(None, "fs"),
        P(),
        P("fs", "tp"),
        P("fs", "tp"),
        P("tp"),
        P("tp"),
        P("tp", "fs"),
        P(None, "fs"),
    )
    return jax.shard_map(
        local, mesh=mesh, in_specs=placed, out_specs=P(("grp", "fs"), "tp"), check_vma=False
    )
```

```python
import functools

import jax
import jax.numpy as jnp
from jax import lax
from jax.experimental import pallas as pl
from jax.experimental.pallas import tpu as pltpu
from jax.sharding import PartitionSpec as P

eps = 1e-06
CORES = 2


def swap_cores(x):
    count = lax.axis_size("tp")
    return lax.ppermute(x, "tp", [(i, i ^ 1) for i in range(count)])


def to_chip(x, step):
    count = lax.axis_size("tp")
    return lax.ppermute(x, "tp", [(i, (i + CORES * step) % count) for i in range(count)])


def from_chips(shard):
    chips = lax.axis_size("tp") // CORES
    return [to_chip(shard, step) for step in range(1, chips)]


def gather_features(shard):
    got = [shard, *from_chips(shard)]
    return [piece for g in got for piece in (g, swap_cores(g))]


def chunk_order(me, count):
    chips = count // CORES
    chip, core = lax.div(me, CORES), lax.rem(me, CORES)
    order = []
    for step in range(chips):
        source = CORES * lax.rem(chip + chips - step, chips)
        order += [source + core, source + 1 - core]
    return order


def chip_sums(mine, theirs):
    other = swap_cores(theirs)
    chips = lax.axis_size("tp") // CORES
    pair = [mine[s].astype(jnp.float32) + other[s].astype(jnp.float32) for s in range(chips)]
    return [pair[0]] + [p.astype(jnp.bfloat16) for p in pair[1:]]


def sum_chips(pair):
    total = pair[0]
    for step, p in enumerate(pair[1:], 1):
        total = total + to_chip(p, step).astype(jnp.float32)
    return total


def dot_f32(a, b, dims=(((1,), (0,)), ((), ()))):
    return lax.dot_general(a, b, dims, preferred_element_type=jnp.float32)


def pass_on(x, step):
    count = lax.axis_size("fs")
    return lax.ppermute(x, "fs", [(i, (i + step) % count) for i in range(count)])


class Ring:
    def __init__(self, shard):
        self.count = lax.axis_size("fs")
        self.ahead = self.behind = shard
        self.held = [shard]
        self.before = [shard, shard]
        self.step = 0

    def advance(self):
        self.step += 1
        before, self.before = self.before, [self.ahead, self.behind]
        self.ahead, _ = lax.optimization_barrier((self.ahead, before[1]))
        self.behind, _ = lax.optimization_barrier((self.behind, before[0]))
        self.ahead = pass_on(self.ahead, 1)
        new = [self.ahead]
        if 2 * self.step < self.count:
            self.behind = pass_on(self.behind, -1)
            new.append(self.behind)
        self.held += new
        return new


def ring_order(me, count):
    order = [me]
    for step in range(1, count // 2 + 1):
        order.append(lax.rem(me + count - step, count))
        if 2 * step < count:
            order.append(lax.rem(me + step, count))
    return order


def lane_block(index, width):
    return pl.ds(pl.multiple_of(index * width, width), width)


def copy_all(pairs, sems, base):
    copies = [
        pltpu.make_async_copy(source, target, sems.at[base + i])
        for i, (source, target) in enumerate(pairs)
    ]
    for copy in copies:
        copy.start()

    def wait():
        for copy in copies:
            copy.wait()

    return wait, base + len(copies)


def load_rows(xs, buf, sems, base):
    width = xs[0].shape[1]
    places = chunk_order(lax.axis_index("tp"), len(xs))
    return copy_all(
        [(x, buf.at[:, lane_block(place, width)]) for x, place in zip(xs, places)], sems, base
    )


def row_factor(x):
    wide = x.astype(jnp.float32)
    return lax.rsqrt(jnp.mean(wide * wide, axis=1, keepdims=True) + eps)


def store_shares(value, weights, chunks, rows, mine_ref, theirs_ref, unroll=False):
    width = mine_ref.shape[2]
    chips = chunks // CORES
    me = lax.axis_index("tp")
    chip, core = lax.div(me, CORES), lax.rem(me, CORES)

    def fill(ref, which):
        def share(step, carry):
            target = CORES * lax.rem(chip + step, chips) + which
            w = weights(lane_block(target, width))
            ref[step, rows, :] = dot_f32(value, w).astype(jnp.bfloat16)
            return carry

        lax.fori_loop(0, chips, share, 0, unroll=unroll)

    fill(mine_ref, core)
    fill(theirs_ref, 1 - core)


def take_rows(xs, places, rows, buf):
    width = xs[0].shape[1]
    squares = None
    for place, x_ref in zip(places, xs):
        x = x_ref[rows, :]
        buf[:, lane_block(place, width)] = x
        wide = x.astype(jnp.float32)
        sq = jnp.sum(wide * wide, axis=1, keepdims=True)
        squares = sq if squares is None else squares + sq
    return lax.rsqrt(squares * (1.0 / (len(xs) * width)) + eps)


def gating_kernel(*refs, chunks, shards, tall):
    xs, ws = refs[:chunks], refs[chunks : chunks + shards]
    spatial_ref, bias_ref, mine_ref, theirs_ref, x_buf, in_buf, out_buf = refs[chunks + shards :]
    span = spatial_ref.shape[0]
    depth = ws[0].shape[0]
    sources = chunk_order(lax.axis_index("tp"), chunks)
    for z, w in zip(ring_order(lax.axis_index("fs"), shards), ws):
        in_buf[lane_block(z, depth), :] = w[:, : 2 * span]
        out_buf[:, lane_block(z, w.shape[1] - 2 * span)] = w[:, 2 * span :]
    later = lax.broadcasted_iota(jnp.int32, (span, span), 0)
    earlier = lax.broadcasted_iota(jnp.int32, (span, span), 1)
    bias = jnp.broadcast_to(bias_ref[...], (span, span)).T
    mixing = spatial_ref[...]
    mixing = jnp.where(later >= earlier, mixing, jnp.zeros_like(mixing))

    def block(i, carry):
        rows = pl.ds(pl.multiple_of(i * tall, tall), tall)
        factor = take_rows(xs, sources, rows, x_buf)
        pre = dot_f32(x_buf[...], in_buf[...]) * factor
        act = 0.5 * pre * (1.0 + lax.erf(pre * (0.5**0.5)))
        u = act[:, :span]
        v = act[:, span:].astype(jnp.bfloat16)
        gated = []
        for b in range(tall // span):
            at = slice(b * span, (b + 1) * span)
            placed = dot_f32(mixing, v[at]) + bias
            gated.append((u[at] * placed).astype(jnp.bfloat16))
        gated = jnp.concatenate(gated, axis=0)
        store_shares(gated, lambda at: out_buf[:, at], chunks, rows, mine_ref, theirs_ref)
        return carry

    lax.fori_loop(0, xs[0].shape[0] // tall, block, 0)


def channel_kernel(*refs, chunks, shards, tall):
    xs, refs = refs[:chunks], refs[chunks:]
    gate_scale_ref, up_scale_ref, far_ref, mine_ref, theirs_ref = refs[:5]
    x_buf, first_buf, down_buf, wide_buf, sems = refs[5:]
    lanes = far_ref.shape[2]
    hidden = down_buf.shape[0]

    def load(part, buf, base):
        rows = slice(part * hidden, (part + 1) * hidden)
        return copy_all(
            [
                (far_ref.at[z, rows, :], buf.at[:, z * lanes : (z + 1) * lanes])
                for z in range(shards)
            ],
            sems,
            base,
        )

    x_here, at = load_rows(xs, x_buf, sems, 0)
    gate_here, at = load(0, first_buf.at[0], at)
    up_here, at = load(1, first_buf.at[1], at)
    down_here, at = load(2, down_buf, at)
    across = (((1,), (1,)), ((), ()))
    blocks = xs[0].shape[0] // tall
    x_here()
    gate_here()

    def project(step, carry):
        pl.when(step == 1)(up_here)

        def block(i, carry):
            rows = pl.ds(pl.multiple_of(i * tall, tall), tall)
            wide_buf[step, rows, :] = dot_f32(x_buf[rows, :], first_buf[step], across)
            return carry

        return lax.fori_loop(0, blocks, block, carry)

    lax.fori_loop(0, 2, project, 0)
    down_here()

    def block(i, carry):
        rows = pl.ds(pl.multiple_of(i * tall, tall), tall)
        factor = row_factor(x_buf[rows, :])
        gate = wide_buf[0, rows, :] * factor * gate_scale_ref[...][None, :]
        up = wide_buf[1, rows, :] * factor * up_scale_ref[...][None, :]
        act = (gate / (1.0 + jnp.exp(-gate)) * up).astype(jnp.bfloat16)
        store_shares(act, lambda at: down_buf[:, at], chunks, rows, mine_ref, theirs_ref, True)
        return carry

    lax.fori_loop(0, blocks, block, 0)


def gain_rows(gain_ref):
    row = gain_ref[pl.ds(lax.axis_index("fs"), 1), :]
    return jnp.broadcast_to(row, (row.shape[1], row.shape[1]))


def fold_kernel(
    in_gain_ref,
    u_ref,
    v_ref,
    mix_ref,
    u_scale_ref,
    v_scale_ref,
    mix_scale_ref,
    mid_gain_ref,
    gate_ref,
    up_ref,
    down_ref,
    down_scale_ref,
    near_ref,
    far_ref,
):
    gain = gain_rows(in_gain_ref).T
    parts = [
        u_ref[...] * gain * u_scale_ref[...],
        v_ref[...] * gain * v_scale_ref[...],
        mix_ref[...] * mix_scale_ref[...],
    ]
    at = 0
    for part in parts:
        near_ref[:, at : at + part.shape[1]] = part.astype(jnp.bfloat16)
        at += part.shape[1]
    gain = gain_rows(mid_gain_ref)[:1, :]
    hidden = gate_ref.shape[0]
    far_ref[:hidden, :] = (gate_ref[...] * gain).astype(jnp.bfloat16)
    far_ref[hidden : 2 * hidden, :] = (up_ref[...] * gain).astype(jnp.bfloat16)
    far_ref[2 * hidden :, :] = (down_ref[...] * down_scale_ref[...]).astype(jnp.bfloat16)


def fold(shapes, *operands):
    return pl.pallas_call(
        fold_kernel,
        grid=(1,),
        in_specs=[pl.BlockSpec(a.shape, lambda i: (0, 0)) for a in operands],
        out_specs=[pl.BlockSpec(memory_space=pltpu.VMEM)] * len(shapes),
        out_shape=[jax.ShapeDtypeStruct(shape, jnp.bfloat16) for shape in shapes],
        cost_estimate=pl.CostEstimate(flops=2**22, bytes_accessed=2**20, transcendentals=0),
        compiler_params=pltpu.CompilerParams(vmem_limit_bytes=60 * 2**20),
        name="fold",
    )(*operands)


def call(kernel, name, operands, specs, chunks, shards, tall, scratch, flops, limit):
    rows, width = operands[0].shape
    half = chunks // CORES
    vmem = pl.BlockSpec(memory_space=pltpu.VMEM)
    return pl.pallas_call(
        functools.partial(kernel, chunks=chunks, shards=shards, tall=tall),
        in_specs=[vmem if spec is None else spec for spec in specs],
        out_specs=[vmem, vmem],
        out_shape=[jax.ShapeDtypeStruct((half, rows, width), jnp.bfloat16)] * 2,
        scratch_shapes=[
            pltpu.VMEM(shape, jnp.bfloat16) if isinstance(shape, tuple) else shape
            for shape in scratch
        ],
        compiler_params=pltpu.CompilerParams(vmem_limit_bytes=limit * 2**20),
        cost_estimate=pl.CostEstimate(flops=flops, bytes_accessed=2**20, transcendentals=0),
        name=name,
    )(*operands)


def gating(pieces, weights, spatial, bias):
    chunks, shards, tall = len(pieces), len(weights), 256
    rows, width = pieces[0].shape
    span = spatial.shape[0]
    model = chunks * width
    flops = 2 * rows * (model * 2 * span + span * span + span * model)
    scratch = [(tall, model), (model, 2 * span), (span, model)]
    operands = [*pieces, *weights, spatial, bias]
    specs = [None] * len(operands)
    return call(gating_kernel, "gating", operands, specs, chunks, shards, tall, scratch, flops, 16)


def channel(pieces, gate_scale, up_scale, far):
    chunks, shards, tall = len(pieces), far.shape[0], 256
    rows, width = pieces[0].shape
    hidden = gate_scale.shape[0]
    model = chunks * width
    flops = 2 * rows * model * 3 * hidden
    scratch = [
        (rows, model),
        (2, hidden, model),
        (hidden, model),
        pltpu.VMEM((2, rows, hidden), jnp.float32),
        pltpu.SemaphoreType.DMA((chunks + 3 * shards,)),
    ]
    operands = [*pieces, gate_scale, up_scale, far]
    specs = [pl.BlockSpec(memory_space=pl.ANY)] * len(operands)
    specs[chunks] = specs[chunks + 1] = None
    return call(channel_kernel, "channel", operands, specs, chunks, shards, tall, scratch, flops, 44)


def local(
    tokens,
    mix_gain,
    w_u,
    w_v,
    u_scale,
    v_scale,
    spatial,
    spatial_bias,
    w_mix,
    mix_scale,
    ffn_gain,
    w_gate,
    w_up,
    gate_scale,
    up_scale,
    w_down,
    down_scale,
):
    depth, span = w_u.shape
    hidden, out = w_down.shape
    near, far = fold(
        [(depth, 2 * span + w_mix.shape[1]), (3 * hidden, out)],
        mix_gain.reshape(-1, depth),
        w_u,
        w_v,
        w_mix,
        u_scale[None],
        v_scale[None],
        mix_scale,
        ffn_gain.reshape(-1, depth),
        w_gate.T,
        w_up.T,
        w_down,
        down_scale,
    )

    far = lax.all_gather(far, "fs")
    ring = Ring(near)
    steps = ring.count // 2
    ring.advance()
    shard, *_ = lax.optimization_barrier((tokens, *ring.advance()))
    got = from_chips(shard)
    while ring.step < steps - 2:
        ring.advance()
    *got, _, _ = lax.optimization_barrier((*got, *ring.held[-2:]))
    other = swap_cores(jnp.stack(got))
    while ring.step < steps:
        ring.advance()
    pieces = [tokens, swap_cores(shard)]
    for i, piece in enumerate(got):
        pieces += [piece, other[i]]
    mine, theirs = gating(pieces, ring.held, spatial[0], spatial_bias)
    resid = (tokens.astype(jnp.float32) + sum_chips(chip_sums(mine, theirs))).astype(jnp.bfloat16)
    mine, theirs = channel(gather_features(resid), gate_scale, up_scale, far)
    pair = chip_sums(mine, theirs)
    return (resid.astype(jnp.float32) + sum_chips(pair)).astype(jnp.bfloat16)


def solution(mesh):
    placed = (
        P(("grp", "fs"), "tp"),
        P(),
        P("fs", "tp"),
        P("fs", "tp"),
        P("tp"),
        P("tp"),
        P("tp", None, None),
        P("tp", None),
        P("tp", "fs"),
        P(None, "fs"),
        P(),
        P("fs", "tp"),
        P("fs", "tp"),
        P("tp"),
        P("tp"),
        P("tp", "fs"),
        P(None, "fs"),
    )
    return jax.shard_map(
        local, mesh=mesh, in_specs=placed, out_specs=P(("grp", "fs"), "tp"), check_vma=False
    )
```
